512 devices in a mesh: sp: 32 (over z, core), tp: 16 (over y, x).
Axes of the slice: x: 4, y: 4, z: 16, core: 2. Of those that a mesh axis runs over, the one named last changes fastest.
Arguments:
- query_rows: bfloat16 [16384, 1024], P('sp', 'tp'), may hold values from -128 to 128
- key_rows: bfloat16 [16384, 1024], P('sp', 'tp'), may hold values from -4 to 4
- value_rows: bfloat16 [16384, 1024], P('sp', 'tp'), may hold values from -6 to 6
- cum_gates: float32 [16384, 16], P('sp', 'tp'), may hold values from -16386 to 0, as said below
- residual: bfloat16 [16384, 2048], P('sp', 'tp'), may hold values from -64 to 64
- output_weight: bfloat16 [1024, 2048], P(None, 'tp'), may hold values from -0.1875 to 0.1875
- norm_gain: bfloat16 [2048], replicated, may hold values from 0.099609375 to 1.8984375
- expert_index: int32 [16384, 2], P('sp'), may hold values from 0 to 31, all different within a row; in each aligned block of 512 rows (0 to 511, 512 to 1023, ...) at most 64 rows name the same one
- route_weights: float32 [16384, 2], P('sp'), may hold values from 0.2 to 1
- gate_weight: bfloat16 [32, 2048, 2048], P('sp', None, 'tp'), may hold values from -2 to 2
- up_weight: bfloat16 [32, 2048, 2048], P('sp', None, 'tp'), may hold values from -2 to 2
- down_weight: bfloat16 [32, 2048, 2048], P('sp', None, 'tp'), may hold values from -0.125 to 0.125
Outputs:
- layer_out: bfloat16 [16384, 2048], P('sp', 'tp')
The draws below stay inside these ranges and needn't reach their ends.
Inputs may be any that keep to these rules, and one draw needn't show every extreme that they name: `cum_gates`: each head's values never rise along positions. `expert_index`: each token names 2 different experts. In the 512 tokens of one index of sp no expert is named more than 64 times, and in some index's tokens some expert is named exactly 64 times.
All inputs are finite; a program needn't handle non-finite values.
Results may differ from the reference program's by a relative error of at most 0.01.
Values may be sent and summed in bfloat16 or wider, within the bound.
A program may use at most 64 MiB of HBM per device.

```python
import math
import jax
import jax.numpy as jnp
import numpy as np
from jax import lax

D = 2048
HEAD_TOTAL = 16
HEAD_DIM = 64
ATT = 1024
FF = 2048
EXPERTS = 32
TOPK = 2
ROWS = 512
SEQUENCE_LENGTH = 16384
CAP = 64


def attention_pair(key):
    base = jax.random.fold_in(key, 101)
    first_key, second_key = jax.random.split(base, 2)
    shape = (SEQUENCE_LENGTH, HEAD_TOTAL, HEAD_DIM)
    key_part = jnp.clip(jax.random.normal(first_key, shape, jnp.float32), -4.0, 4.0)
    query_part = jnp.clip(3.0 * jax.random.normal(second_key, shape, jnp.float32), -12.0, 12.0)
    return (query_part.reshape(SEQUENCE_LENGTH, HEAD_TOTAL * HEAD_DIM), key_part.reshape(SEQUENCE_LENGTH, HEAD_TOTAL * HEAD_DIM))


def draw_query_rows(key, part):
    return attention_pair(key)[0].astype(jnp.bfloat16)


def draw_key_rows(key, part):
    return attention_pair(key)[1].astype(jnp.bfloat16)


def draw_cum_gates(key, part):
    base = jax.random.fold_in(key, 202)
    ordering, ranking, texture, token_positions, depths = jax.random.split(base, 5)
    order = jax.random.permutation(ordering, HEAD_TOTAL)
    sluggish_decay = order >= HEAD_TOTAL // 2
    rough = jax.random.uniform(texture, (SEQUENCE_LENGTH, HEAD_TOTAL), jnp.float32, 0.4, 1.6)
    blocks = SEQUENCE_LENGTH // ROWS
    ladder = jax.random.permutation(ranking, blocks).astype(jnp.float32) / max(blocks - 1, 1)
    factor = jnp.repeat(0.5 * 4.0 ** ladder, ROWS)
    rate = jnp.where(sluggish_decay, 0.8 / SEQUENCE_LENGTH, 1.0 / min(40.0, ROWS / 2.0))
    forget_steps = -factor[:, None] * rate[None, :] * rough
    spike_position = jax.random.randint(token_positions, (HEAD_TOTAL, 2), 0, SEQUENCE_LENGTH)
    decay_drops = jax.random.uniform(depths, (HEAD_TOTAL, 2), jnp.float32, math.log(0.5), math.log(0.8))
    head_ordinal = jnp.broadcast_to(jnp.arange(HEAD_TOTAL, dtype=jnp.int32)[:, None], (HEAD_TOTAL, 2))
    spike_events = jnp.zeros((SEQUENCE_LENGTH, HEAD_TOTAL), jnp.float32).at[spike_position, head_ordinal].add(decay_drops * sluggish_decay[:, None].astype(jnp.float32))
    return jnp.cumsum(forget_steps + spike_events, axis=0)


def draw_residual(key, part):
    base = jax.random.fold_in(key, 303)
    values_key = jax.random.fold_in(base, 0)
    place = jnp.arange(D, dtype=jnp.float32) / D - 0.5
    noise = jnp.clip(jax.random.normal(values_key, (SEQUENCE_LENGTH, D), jnp.float32), -6.0, 6.0)
    rising = jnp.exp(math.log(3.0) * place)
    return (noise * rising[None, :]).astype(jnp.bfloat16)


def expert_matrix(key, salt):
    base = jax.random.fold_in(key, salt)
    values_key, column_key = jax.random.split(base, 2)
    shape = (EXPERTS, D, FF)
    noise = jnp.clip(jax.random.normal(values_key, shape, jnp.float32), -6.0, 6.0)
    column = jnp.exp(jax.random.uniform(column_key, (EXPERTS, 1, FF), jnp.float32, 0.0, math.log(3.0)))
    return jnp.clip(noise * column / math.sqrt(D), -2.0, 2.0).astype(jnp.bfloat16)


def draw_gate_weight(key, part):
    return expert_matrix(key, 404)


def draw_up_weight(key, part):
    return expert_matrix(key, 505)


def levels(key, extent, cuts, least, largest):
    factor_of, own = 1.0, jax.random.fold_in(key, 6)
    for position, shards_of in cuts:
        steps = jnp.exp(jax.random.uniform(jax.random.fold_in(own, position), (shards_of,), jnp.float32, least / len(cuts), largest / len(cuts)))
        factor_of = factor_of * jnp.repeat(steps, extent[position] // shards_of).reshape([-1 if axis == position else 1 for axis in range(len(extent))])
    return factor_of


def shared_out(rng, own, number, rows, count, top, most, slope):
    order = jax.random.permutation(rng, count)
    crowded, ordinary = portions_of(count, rows * top, most, slope, True), portions_of(count, rows * top, most, slope, False)
    places = jnp.arange(count)

    def named(lengths, offset_by):
        used = int((lengths > 0).sum())
        fixed = max(1, used // 4)
        passed = fixed + (places - fixed + offset_by * (used - fixed)) % max(1, count - fixed)
        return jnp.zeros((count,), jnp.int32).at[order[jnp.where(places < fixed, places, passed)]].set(jnp.asarray(lengths, jnp.int32))

    lengths = jnp.where(number % 4 == 0, named(crowded, number // 4), named(ordinary, number - number // 4 - 1))
    mixed = jax.random.permutation(jax.random.fold_in(own, 3), count)
    source_of, taker = mixed[0:count // 2 * 2:2], mixed[1:count // 2 * 2:2]
    margin = jnp.minimum(lengths[source_of] - 1, most - lengths[taker]) // 2
    margin = jnp.where((source_of == order[0]) | (taker == order[0]) | (lengths[taker] == 0), 0, jnp.maximum(margin, 0))
    passed = jax.random.randint(jax.random.fold_in(own, 4), (count // 2,), 0, 1 << 20) % (margin + 1)
    lengths = lengths.at[source_of].add(-passed).at[taker].add(passed)
    members = jnp.searchsorted(jnp.cumsum(lengths), jnp.arange(rows * top), side="right").astype(jnp.int32)
    table = members.reshape(top, rows).T
    table = table[jax.random.permutation(jax.random.fold_in(own, 1), rows)]
    offset_by = jax.random.randint(jax.random.fold_in(own, 2), (rows, 1), 0, top)
    return jnp.take_along_axis(table, (jnp.arange(top)[None, :] + offset_by) % top, axis=1)


def portions_of(number_of, total, limit, lean, full):
    portions = [(1 << 20) // math.isqrt(standing ** lean) + 1 for standing in range(1, number_of + 1)]
    largest = limit if full else min(limit, max(-(-total // number_of), total * portions[0] // sum(portions)))
    least = 1 if total - largest >= number_of - 1 else 0
    counts, spare = [largest] + [least] * (number_of - 1), total - largest - least * (number_of - 1)
    while spare > 0:
        free = [i for i in range(1, number_of) if counts[i] < largest] or [i for i in range(1, number_of) if counts[i] < limit]
        mass, budget = sum([portions[i] for i in free]), spare
        for i in free:
            extra = min(limit - counts[i], max(1, budget * portions[i] // mass), spare)
            counts[i] = counts[i] + extra
            spare = spare - extra
    return np.array(counts)


def normal_values(rng, dims, spread, most, pieces=(), held_as=jnp.bfloat16):
    level = levels(rng, dims, pieces, -0.22, 0.18) if pieces else 1.0
    values = jax.random.normal(rng, dims, jnp.float32) * spread * level
    return jnp.minimum(jnp.maximum(values, -most), most).astype(held_as)


def setup_inputs(seed: int = 0) -> dict:
    streams_of = jax.random.split(jax.random.key(seed), 13)
    query_rows = draw_query_rows(jax.random.fold_in(streams_of[12], 71), 0)
    key_rows = draw_key_rows(jax.random.fold_in(streams_of[12], 71), 0)
    value_rows = normal_values(streams_of[2], (SEQUENCE_LENGTH, ATT), 1.0, 6.0, ((0, 32), (1, 16)))
    cum_gates = draw_cum_gates(jax.random.fold_in(streams_of[12], 71), 0)
    residual = draw_residual(jax.random.fold_in(streams_of[12], 71), 0)
    output_weight = normal_values(streams_of[5], (ATT, D), ATT ** -0.5, 0.1875, ((1, 16),))
    norm_gain = jnp.clip(1.0 + 0.18 * jax.random.normal(streams_of[6], (D,), jnp.float32), 0.099609375, 1.8984375).astype(jnp.bfloat16)
    expert_index_keys = jax.random.split(jax.random.fold_in(streams_of[7], 1), SEQUENCE_LENGTH // ROWS)
    expert_index_turns = jax.random.permutation(jax.random.fold_in(streams_of[7], 3), SEQUENCE_LENGTH // ROWS)
    expert_index = jax.vmap(lambda own, number: shared_out(jax.random.fold_in(streams_of[7], 2), own, number, ROWS, EXPERTS, TOPK, CAP, 2))(expert_index_keys, expert_index_turns).reshape((SEQUENCE_LENGTH, TOPK))
    route_weights = jnp.clip(0.2 + 0.8 * jax.random.uniform(streams_of[8], (SEQUENCE_LENGTH, TOPK), jnp.float32) ** levels(streams_of[8], (SEQUENCE_LENGTH, TOPK), ((0, 32),), -0.2, 0.2), 0.2, 1.0)
    gate_weight = draw_gate_weight(jax.random.fold_in(streams_of[12], 71), 0)
    up_weight = draw_up_weight(jax.random.fold_in(streams_of[12], 71), 0)
    down_weight = normal_values(streams_of[11], (EXPERTS, FF, D), FF ** -0.5, 0.125, ((0, 32), (2, 16)))
    return dict(query_rows=query_rows, key_rows=key_rows, value_rows=value_rows, cum_gates=cum_gates, residual=residual, output_weight=output_weight, norm_gain=norm_gain, expert_index=expert_index, route_weights=route_weights, gate_weight=gate_weight, up_weight=up_weight, down_weight=down_weight)


NORM_EPS = 1e-06
CLAMP_LIMIT = 7.0
SILU_ALPHA = 1.702

def attend(query_rows, key_rows, value_rows, cum_gates):
    length = query_rows.shape[0]
    heads = cum_gates.shape[1]
    head_size = query_rows.shape[1] // heads
    queries = query_rows.reshape(length, heads, head_size)
    key_heads = key_rows.reshape(length, heads, head_size).astype(jnp.float32)
    value_heads = value_rows.reshape(length, heads, head_size).astype(jnp.float32)
    block = math.gcd(length, 512)
    positions = jnp.arange(length, dtype=jnp.int32)

    def one_block(number):
        start = number * block
        query_block = lax.dynamic_slice_in_dim(queries, start, block, 0).astype(jnp.float32)
        query_gates = lax.dynamic_slice_in_dim(cum_gates, start, block, 0)
        scores = jnp.einsum('qhd,khd->hqk', query_block, key_heads) * head_size ** (-0.5)
        scores = scores + query_gates.T[:, :, None] - cum_gates.T[:, None, :]
        query_place = start + jnp.arange(block, dtype=jnp.int32)
        allowed = positions[None, :] <= query_place[:, None]
        scores = jnp.where(allowed[None], scores, -jnp.inf)
        top = lax.optimization_barrier(jnp.max(scores, axis=-1, keepdims=True))
        raised = jnp.exp(scores - top)
        total = lax.optimization_barrier(jnp.sum(raised, axis=-1))
        weights = raised.astype(jnp.bfloat16).astype(jnp.float32)
        summed = jnp.einsum('hqk,khd->qhd', weights, value_heads)
        return (summed / total.T[:, :, None]).astype(jnp.bfloat16).reshape(block, heads * head_size)
    return lax.map(one_block, jnp.arange(length // block, dtype=jnp.int32)).reshape(length, heads * head_size)

def expert_rows(rows, gate_part, up_part, down_part):
    gate_input = jnp.dot(rows, gate_part, preferred_element_type=jnp.float32)
    linear_input = jnp.dot(rows, up_part, preferred_element_type=jnp.float32)
    gate_cut = jnp.minimum(gate_input, CLAMP_LIMIT)
    linear_cut = jnp.clip(linear_input, -CLAMP_LIMIT, CLAMP_LIMIT)
    activated = (gate_cut * jax.nn.sigmoid(SILU_ALPHA * gate_cut) * (linear_cut + 1.0)).astype(jnp.bfloat16)
    return jnp.dot(activated, down_part, preferred_element_type=jnp.float32).astype(jnp.bfloat16)

def reference(query_rows, key_rows, value_rows, cum_gates, residual, output_weight, norm_gain, expert_index, route_weights, gate_weight, up_weight, down_weight):
    attended = attend(query_rows, key_rows, value_rows, cum_gates)
    mixed = (residual.astype(jnp.float32) + jnp.dot(attended, output_weight, preferred_element_type=jnp.float32)).astype(jnp.bfloat16)
    wide = mixed.astype(jnp.float32)
    factor = lax.rsqrt(lax.optimization_barrier(jnp.mean(wide * wide, axis=-1, keepdims=True)) + NORM_EPS)
    normed = (wide * factor * norm_gain.astype(jnp.float32)).astype(jnp.bfloat16)
    experts = gate_weight.shape[0]
    blocks = SEQUENCE_LENGTH // ROWS
    chosen = expert_index.reshape(blocks, ROWS * TOPK)
    matches = (chosen[:, :, None] == jnp.arange(experts, dtype=jnp.int32)[None, None, :]).astype(jnp.int32)
    rank = lax.optimization_barrier(jnp.sum((jnp.cumsum(matches, axis=1) - matches) * matches, axis=2))
    slot = jnp.arange(blocks, dtype=jnp.int32)[:, None] * CAP + rank
    owner = jnp.arange(blocks * ROWS * TOPK, dtype=jnp.int32).reshape(blocks, ROWS * TOPK) // TOPK
    table = jnp.full((experts, blocks * CAP), SEQUENCE_LENGTH, jnp.int32).at[chosen, slot].set(owner)
    padded = jnp.concatenate([normed, jnp.zeros((1, D), normed.dtype)], axis=0)

    def one_expert(number):
        rows = padded[table[number]]
        return expert_rows(rows, gate_weight[number], up_weight[number], down_weight[number])
    outputs = lax.map(one_expert, jnp.arange(experts, dtype=jnp.int32))
    picked = outputs[chosen, slot].reshape(SEQUENCE_LENGTH, TOPK, D).astype(jnp.float32)
    blended = lax.optimization_barrier(jnp.sum(route_weights[:, :, None] * picked, axis=1))
    return (mixed.astype(jnp.float32) + blended).astype(jnp.bfloat16)
```

```python
import functools
import math

import jax
import jax.numpy as jnp
from jax import lax
from jax.experimental import pallas as pl
from jax.experimental.pallas import tpu as pltpu
from jax.sharding import PartitionSpec as P

NORM_EPS = 1e-06
CLAMP_LIMIT = 7.0
SILU_ALPHA = 1.702
MESH = pl.DeviceIdType.MESH
GATE_ROWS = 16


def remote(src, dst, send_sem, recv_sem, **where):
    return pltpu.make_async_remote_copy(
        src_ref=src,
        dst_ref=dst,
        send_sem=send_sem,
        recv_sem=recv_sem,
        device_id=where,
        device_id_type=MESH,
    )


def attention_kernel(
    sp_size,
    tp_size,
    q_ref,
    k_ref,
    v_ref,
    gate_ref,
    residual_ref,
    weight_ref,
    mixed_ref,
    kv_all,
    qpad,
    wide,
    top,
    total,
    summed,
    att_all,
    kv_recv,
    own_recv,
    ring_send,
    pair_send,
    att_recv,
    att_send,
):
    chips = sp_size // 2
    ups = chips // 2
    downs = chips - 1 - ups
    sp = lax.axis_index("sp")
    tp = lax.axis_index("tp")
    chip = sp // 2
    core = sp - 2 * chip
    rows, size = q_ref.shape
    half = rows // 2
    cut = (GATE_ROWS + rows) // 2
    up_sp = lax.rem(chip + 1, chips) * 2 + core
    down_sp = lax.rem(chip + chips - 1, chips) * 2 + core
    pair_sp = chip * 2 + 1 - core

    barrier = pltpu.get_barrier_semaphore()
    for target in (up_sp, down_sp, pair_sp):
        pl.semaphore_signal(barrier, inc=1, device_id={"sp": target}, device_id_type=MESH)
    for d in range(1, tp_size):
        pl.semaphore_signal(
            barrier, inc=1, device_id={"tp": lax.rem(tp + d, tp_size)}, device_id_type=MESH
        )

    gates = gate_ref[...]
    high = gates.astype(jnp.bfloat16)
    rest = gates - high.astype(jnp.float32)
    middle = rest.astype(jnp.bfloat16)
    low = (rest - middle.astype(jnp.float32)).astype(jnp.bfloat16)
    kv_all[sp, 0:GATE_ROWS, :] = jnp.concatenate(
        [
            high.astype(jnp.float32),
            middle.astype(jnp.float32),
            low.astype(jnp.float32),
            jnp.zeros_like(gates),
        ],
        axis=0,
    ).astype(jnp.bfloat16)
    kv_all[sp, GATE_ROWS:, :] = jnp.concatenate([k_ref[...], v_ref[...]], axis=1)
    qs = (q_ref[...].astype(jnp.float32) * (size**-0.5)).astype(jnp.bfloat16)
    qpad[...] = jnp.concatenate([qs, jnp.zeros_like(qs)], axis=1)
    first_gate = gates[0:1, 0:1]

    pl.semaphore_wait(barrier, 3 + tp_size - 1)

    def piece(slot, part):
        return kv_all.at[slot, pl.ds(part * cut, cut), :]

    def hop(slot, step, way, part, target):
        return remote(
            piece(slot, part),
            piece(slot, part),
            ring_send.at[step, way, part],
            kv_recv.at[slot, part],
            sp=target,
        )

    def share(slot, step, way):
        return remote(
            kv_all.at[slot],
            kv_all.at[slot],
            pair_send.at[step, way],
            own_recv.at[slot],
            sp=pair_sp,
        )

    if ups >= 1:
        for part in range(2):
            hop(sp, 0, 0, part, up_sp).start()
            if downs >= 1:
                hop(sp, 0, 1, part, down_sp).start()
    share(sp, 0, 0).start()

    wide[...] = jnp.zeros_like(wide)
    for h in range(tp_size):
        w = weight_ref[h * size : (h + 1) * size, :]
        wide[h * 2 * size : h * 2 * size + size, 0 : w.shape[1]] = w
        wide[h * 2 * size + size : (h + 1) * 2 * size, w.shape[1] :] = w

    top[...] = jnp.full_like(top, -1e30)
    total[...] = jnp.zeros_like(total)
    summed[...] = jnp.zeros_like(summed)
    tile = min(128, rows)
    lanes = 128

    def attend(slot, diagonal):
        parts = kv_all[slot, 0:GATE_ROWS, :].astype(jnp.float32)
        n4 = GATE_ROWS // 4
        key_gates = parts[0:n4] + parts[n4 : 2 * n4] + parts[2 * n4 : 3 * n4]
        shift = first_gate - key_gates
        keys = kv_all[slot, GATE_ROWS:, :]
        for t in range(rows // tile):
            here = slice(t * tile, (t + 1) * tile)
            scores = lax.dot_general(
                qpad[here, :], keys, (((1,), (1,)), ((), ())), preferred_element_type=jnp.float32
            )
            pieces = []
            for j in range(rows // lanes):
                s = scores[:, j * lanes : (j + 1) * lanes] + shift[j : j + 1, :]
                if diagonal:
                    place = lax.broadcasted_iota(jnp.int32, s.shape, 0) + t * tile
                    other = lax.broadcasted_iota(jnp.int32, s.shape, 1) + j * lanes
                    s = jnp.where(other <= place, s, -1e30)
                pieces.append(s)
            most = functools.reduce(jnp.maximum, pieces)
            old = top[here, :]
            new = jnp.maximum(old, jnp.max(most, axis=1, keepdims=True))
            shrink = jnp.exp(old - new)
            raised = [jnp.exp(s - new) for s in pieces]
            total[here, :] = total[here, :] * shrink + functools.reduce(jnp.add, raised)
            weights = jnp.concatenate([r.astype(jnp.bfloat16) for r in raised], axis=1)
            summed[here, :] = summed[here, :] * shrink + jnp.dot(
                weights, keys, preferred_element_type=jnp.float32
            )
            top[here, :] = new

    attend(sp, True)

    def earlier(slot):
        @pl.when(slot < sp)
        def _():
            attend(slot, False)

    def slots(step):
        up_from = lax.rem(chip + chips - step, chips)
        down_from = lax.rem(chip + step, chips)
        return up_from, down_from

    def arrive(slot, step, way, part, target, send):
        hop(slot, step, way, part, target).wait_recv()
        if send is True:
            hop(slot, step, way, part, target).start()
        elif send is not False:

            @pl.when(send)
            def _():
                hop(slot, step, way, part, target).start()

    def partner(step, way, slot):
        share(slot, step, way).wait_recv()
        earlier(slot)

    def both(step):
        up_from, down_from = slots(step)
        before_up, before_down = slots(step - 1)
        up_slot, down_slot = up_from * 2 + core, down_from * 2 + core
        for part in range(2):
            arrive(up_slot, step, 0, part, up_sp, step < ups)
        share(up_slot, step, 0).start()
        earlier(up_slot)
        for part in range(2):
            arrive(down_slot, step, 1, part, down_sp, step < downs)
        share(down_slot, step, 1).start()
        earlier(down_slot)
        partner(step - 1, 0, before_up * 2 + 1 - core)

        @pl.when(step >= 2)
        def _():
            partner(step - 1, 1, before_down * 2 + 1 - core)

    if downs >= 1:
        lax.fori_loop(1, downs + 1, lambda i, c: (both(i), c)[1], 0)
    last_up, last_down = slots(downs)
    up_from, _ = slots(ups)
    up_slot = up_from * 2 + core
    for part in range(2):
        arrive(up_slot, ups, 0, part, up_sp, False)
    share(up_slot, ups, 0).start()
    earlier(up_slot)
    partner(downs, 0, last_up * 2 + 1 - core)
    if downs >= 1:
        partner(downs, 1, last_down * 2 + 1 - core)
    partner(ups, 0, up_from * 2 + 1 - core)

    def finished(lo):
        here = slice(lo, lo + half)
        whole = jnp.sum(total[here, :], axis=1, keepdims=True)
        return summed[here, :] / whole

    left = pltpu.roll(finished(0), size, 1)
    right = finished(half)
    lane = lax.broadcasted_iota(jnp.int32, left.shape, 1)
    att_all[tp] = jnp.where(lane < size, left, right).astype(jnp.bfloat16)

    def give(d):
        return remote(
            att_all.at[tp],
            att_all.at[tp],
            att_send.at[d],
            att_recv.at[tp],
            tp=lax.rem(tp + d, tp_size),
        )

    def take(d):
        owner = lax.rem(tp + tp_size - d, tp_size)
        return remote(
            att_all.at[owner],
            att_all.at[owner],
            att_send.at[d],
            att_recv.at[owner],
            tp=owner,
        )

    for d in range(1, tp_size):
        give(d).start()
    for d in range(1, tp_size):
        take(d).wait_recv()
    projected = jnp.zeros((half, wide.shape[1]), jnp.float32)
    for j in range(tp_size // 2):
        pair = jnp.concatenate([att_all[2 * j], att_all[2 * j + 1]], axis=1)
        projected += jnp.dot(
            pair, wide[j * 4 * size : (j + 1) * 4 * size, :], preferred_element_type=jnp.float32
        )
    columns = weight_ref.shape[1]
    for part in range(2):
        here = slice(part * half, (part + 1) * half)
        mixed_ref[here, :] = (
            residual_ref[here, :].astype(jnp.float32)
            + projected[:, part * columns : (part + 1) * columns]
        ).astype(jnp.bfloat16)

    if ups >= 1:
        for step in range(ups):
            for part in range(2):
                hop(sp, step, 0, part, up_sp).wait_send()
        for step in range(downs):
            for part in range(2):
                hop(sp, step, 1, part, down_sp).wait_send()
        for step in range(1, ups + 1):
            share(sp, step, 0).wait_send()
        for step in range(1, downs + 1):
            share(sp, step, 1).wait_send()
    share(sp, 0, 0).wait_send()
    for d in range(1, tp_size):
        give(d).wait_send()


def attention(mesh, query_rows, key_rows, value_rows, cum_gates, residual, output_weight):
    sp_size, tp_size = mesh.shape["sp"], mesh.shape["tp"]
    rows, size = query_rows.shape
    columns = output_weight.shape[1]
    vmem = pl.BlockSpec(memory_space=pltpu.VMEM)
    chips = sp_size // 2
    steps = chips // 2 + 1
    return pl.pallas_call(
        functools.partial(attention_kernel, sp_size, tp_size),
        out_shape=jax.ShapeDtypeStruct((rows, columns), jnp.bfloat16),
        in_specs=[vmem] * 6,
        out_specs=vmem,
        scratch_shapes=[
            pltpu.VMEM((sp_size, GATE_ROWS + rows, 2 * size), jnp.bfloat16),
            pltpu.VMEM((rows, 2 * size), jnp.bfloat16),
            pltpu.VMEM((tp_size * 2 * size, 2 * columns), jnp.bfloat16),
            pltpu.VMEM((rows, 2 * size), jnp.float32),
            pltpu.VMEM((rows, 2 * size), jnp.float32),
            pltpu.VMEM((rows, 2 * size), jnp.float32),
            pltpu.VMEM((tp_size, rows // 2, 2 * size), jnp.bfloat16),
            pltpu.SemaphoreType.DMA((sp_size, 2)),
            pltpu.SemaphoreType.DMA((sp_size,)),
            pltpu.SemaphoreType.DMA((steps, 2, 2)),
            pltpu.SemaphoreType.DMA((steps, 2)),
            pltpu.SemaphoreType.DMA((tp_size,)),
            pltpu.SemaphoreType.DMA((tp_size,)),
        ],
        compiler_params=pltpu.CompilerParams(
            collective_id=0, has_side_effects=True, vmem_limit_bytes=40 << 20
        ),
        cost_estimate=pl.CostEstimate(
            flops=4 * rows * rows * sp_size * 2 * size,
            bytes_accessed=1 << 22,
            transcendentals=rows * rows * sp_size,
        ),
    )(
        query_rows,
        key_rows,
        value_rows,
        cum_gates.reshape(4, rows // 4),
        residual,
        output_weight,
    )


def normalize(rows, norm_gain):
    wide = rows.astype(jnp.float32)
    factor = lax.rsqrt(jnp.mean(wide * wide, axis=-1, keepdims=True) + NORM_EPS)
    return (wide * factor * norm_gain.astype(jnp.float32)).astype(jnp.bfloat16)


def body(
    mesh,
    query_rows,
    key_rows,
    value_rows,
    cum_gates,
    residual,
    output_weight,
    norm_gain,
    expert_index,
    route_weights,
    gate_weight,
    up_weight,
    down_weight,
):
    mixed = attention(
        mesh, query_rows, key_rows, value_rows, cum_gates, residual, output_weight
    )
    rows = residual.shape[0]
    topk = expert_index.shape[1]
    local_experts = gate_weight.shape[0]
    groups = lax.axis_size("sp")
    experts = local_experts * groups
    capacity = 2 * rows * topk // experts
    chosen = expert_index.reshape(rows * topk)
    matches = (chosen[:, None] == jnp.arange(experts, dtype=jnp.int32)[None, :]).astype(jnp.int32)
    rank = jnp.sum((jnp.cumsum(matches, axis=0) - matches) * matches, axis=1)
    slot = chosen * capacity + rank
    owner = jnp.arange(rows * topk, dtype=jnp.int32) // topk
    slot_token = jnp.full((experts * capacity,), rows, jnp.int32).at[slot].set(owner)
    padded = jnp.concatenate([mixed, jnp.zeros((1, mixed.shape[1]), mixed.dtype)], axis=0)
    outgoing = padded[slot_token].reshape(experts, capacity, mixed.shape[1])
    arrived = lax.all_to_all(outgoing, "sp", split_axis=0, concat_axis=0, tiled=True)
    count = arrived.shape[1]
    grouped = arrived.reshape(groups, local_experts, count, arrived.shape[2])
    normed = normalize(lax.all_gather(grouped, "tp", axis=3, tiled=True), norm_gain)
    gate_input = jnp.einsum(
        "seid,edf->seif", normed, gate_weight, preferred_element_type=jnp.float32
    )
    linear_input = jnp.einsum(
        "seid,edf->seif", normed, up_weight, preferred_element_type=jnp.float32
    )
    gate_cut = jnp.minimum(gate_input, CLAMP_LIMIT)
    linear_cut = jnp.clip(linear_input, -CLAMP_LIMIT, CLAMP_LIMIT)
    activated = (gate_cut * jax.nn.sigmoid(SILU_ALPHA * gate_cut) * (linear_cut + 1.0)).astype(
        jnp.bfloat16
    )
    weight_rows = down_weight
    produced = jnp.einsum(
        "seif,efc->seic",
        lax.all_gather(activated, "tp", axis=3, tiled=True),
        weight_rows,
        preferred_element_type=jnp.float32,
    ).astype(jnp.bfloat16)
    returned = lax.all_to_all(
        produced.reshape(groups * local_experts, count, down_weight.shape[2]),
        "sp",
        split_axis=0,
        concat_axis=0,
        tiled=True,
    )
    flat = returned.reshape(experts * capacity, returned.shape[2])
    picked = flat[slot].reshape(rows, topk, flat.shape[1]).astype(jnp.float32)
    blended = jnp.sum(route_weights[:, :, None] * picked, axis=1)
    return (mixed.astype(jnp.float32) + blended).astype(jnp.bfloat16)


def solution(mesh):
    placed = (
        P("sp", "tp"),
        P("sp", "tp"),
        P("sp", "tp"),
        P("sp", "tp"),
        P("sp", "tp"),
        P(None, "tp"),
        P(),
        P("sp", None),
        P("sp", None),
        P("sp", None, "tp"),
        P("sp", None, "tp"),
        P("sp", None, "tp"),
    )
    return jax.shard_map(
        functools.partial(body, mesh), mesh=mesh, in_specs=placed, out_specs=P("sp", "tp"), check_vma=False)
```

```python
import functools
import math

import jax
import jax.numpy as jnp
from jax import lax
from jax.experimental import pallas as pl
from jax.experimental.pallas import tpu as pltpu
from jax.sharding import PartitionSpec as P

NORM_EPS = 1e-06
CLAMP_LIMIT = 7.0
SILU_ALPHA = 1.702
MESH = pl.DeviceIdType.MESH
GATE_ROWS = 16


def remote(src, dst, send_sem, recv_sem, **where):
    return pltpu.make_async_remote_copy(
        src_ref=src,
        dst_ref=dst,
        send_sem=send_sem,
        recv_sem=recv_sem,
        device_id=where,
        device_id_type=MESH,
    )


def ring_start(n, place, make):
    if n == 4:
        for k in range(2):
            make(place, k, 1, 0, k).start()
            make(place, 1 - k, 3, 1, k).start()
    elif n == 2:
        for k in range(2):
            make(place, k, 1, 0, k).start()


def ring_forward(n, place, make):
    if n == 4:
        before, after = lax.rem(place + 3, 4), lax.rem(place + 1, 4)
        make(before, 0, 1, 0, 2).wait_recv()
        make(before, 0, 1, 0, 2).start()
        make(after, 1, 3, 1, 2).wait_recv()
        make(after, 1, 3, 1, 2).start()


def ring_finish(n, place, make):
    if n == 4:
        make(lax.rem(place + 3, 4), 1, 1, 0, 0).wait_recv()
        make(lax.rem(place + 1, 4), 0, 1, 0, 0).wait_recv()
        for k in range(2):
            make(lax.rem(place + 2, 4), k, 1, 0, 0).wait_recv()
    elif n == 2:
        for k in range(2):
            make(1 - place, k, 1, 0, 0).wait_recv()


def ring_sent(n, place, make):
    if n == 4:
        for k in range(3):
            half = k if k < 2 else 0
            make(place, half, 1, 0, k).wait_send()
            make(place, 1 - half, 3, 1, k).wait_send()
    elif n == 2:
        for k in range(2):
            make(place, k, 1, 0, k).wait_send()


def attention_kernel(
    sp_size,
    tp_size,
    y_size,
    q_ref,
    k_ref,
    v_ref,
    gate_ref,
    residual_ref,
    weight_ref,
    gate_w,
    up_w,
    down_w,
    mixed_ref,
    gate_all,
    up_all,
    down_all,
    kv_all,
    qpad,
    wide,
    top,
    total,
    summed,
    att_all,
    kv_recv,
    own_recv,
    ring_send,
    pair_send,
    att_recv,
    att_send,
    own_w,
    w_recv,
    w_send,
):
    chips = sp_size // 2
    ups = chips // 2
    downs = chips - 1 - ups
    sp = lax.axis_index("sp")
    tp = lax.axis_index("tp")
    chip = sp // 2
    core = sp - 2 * chip
    rows, size = q_ref.shape
    half = rows // 2
    cut = (GATE_ROWS + rows) // 2
    up_sp = lax.rem(chip + 1, chips) * 2 + core
    down_sp = lax.rem(chip + chips - 1, chips) * 2 + core
    pair_sp = chip * 2 + 1 - core

    barrier = pltpu.get_barrier_semaphore()
    for target in (up_sp, down_sp, pair_sp):
        pl.semaphore_signal(barrier, inc=1, device_id={"sp": target}, device_id_type=MESH)
    for d in range(1, tp_size):
        pl.semaphore_signal(
            barrier, inc=1, device_id={"tp": lax.rem(tp + d, tp_size)}, device_id_type=MESH
        )

    gates = gate_ref[...]
    high = gates.astype(jnp.bfloat16)
    rest = gates - high.astype(jnp.float32)
    middle = rest.astype(jnp.bfloat16)
    low = (rest - middle.astype(jnp.float32)).astype(jnp.bfloat16)
    kv_all[sp, 0:GATE_ROWS, :] = jnp.concatenate(
        [
            high.astype(jnp.float32),
            middle.astype(jnp.float32),
            low.astype(jnp.float32),
            jnp.zeros_like(gates),
        ],
        axis=0,
    ).astype(jnp.bfloat16)
    kv_all[sp, GATE_ROWS:, :] = jnp.concatenate([k_ref[...], v_ref[...]], axis=1)
    qs = (q_ref[...].astype(jnp.float32) * (size**-0.5)).astype(jnp.bfloat16)
    qpad[...] = jnp.concatenate([qs, jnp.zeros_like(qs)], axis=1)
    first_gate = gates[0:1, 0:1]

    pl.semaphore_wait(barrier, 3 + tp_size - 1)

    def piece(slot, part):
        return kv_all.at[slot, pl.ds(part * cut, cut), :]

    def hop(slot, step, way, part, target):
        return remote(
            piece(slot, part),
            piece(slot, part),
            ring_send.at[step, way, part],
            kv_recv.at[slot, part],
            sp=target,
        )

    def share(slot, step, way):
        return remote(
            kv_all.at[slot],
            kv_all.at[slot],
            pair_send.at[step, way],
            own_recv.at[slot],
            sp=pair_sp,
        )

    x_size = tp_size // y_size
    y = tp // x_size
    x = tp - y * x_size
    matrices = ((gate_w, gate_all), (up_w, up_all), (down_w, down_all))
    depth = gate_w.shape[1]

    def weight_copy(m):
        own, every = matrices[m]

        def make(owner, k, step, way, index):
            here = every.at[owner, pl.ds(k * (depth // 2), depth // 2), :]
            mine = own.at[0, pl.ds(k * (depth // 2), depth // 2), :]
            return remote(
                mine if index < 2 else here,
                here,
                w_send.at[m, way, index],
                w_recv.at[m, owner, k],
                tp=lax.rem(y + step, y_size) * x_size + x,
            )

        return make

    locals_w = [
        pltpu.make_async_copy(own.at[0], every.at[y], own_w.at[m])
        for m, (own, every) in enumerate(matrices)
    ]

    if ups >= 1:
        for part in range(2):
            hop(sp, 0, 0, part, up_sp).start()
            if downs >= 1:
                hop(sp, 0, 1, part, down_sp).start()
    share(sp, 0, 0).start()
    for m in range(3):
        ring_start(y_size, y, weight_copy(m))
        locals_w[m].start()

    wide[...] = jnp.zeros_like(wide)
    for h in range(tp_size):
        w = weight_ref[h * size : (h + 1) * size, :]
        wide[h * 2 * size : h * 2 * size + size, 0 : w.shape[1]] = w
        wide[h * 2 * size + size : (h + 1) * 2 * size, w.shape[1] :] = w

    top[...] = jnp.full_like(top, -1e30)
    total[...] = jnp.zeros_like(total)
    summed[...] = jnp.zeros_like(summed)
    tile = min(128, rows)
    lanes = 128

    def attend(slot, diagonal):
        parts = kv_all[slot, 0:GATE_ROWS, :].astype(jnp.float32)
        n4 = GATE_ROWS // 4
        key_gates = parts[0:n4] + parts[n4 : 2 * n4] + parts[2 * n4 : 3 * n4]
        shift = first_gate - key_gates
        keys = kv_all[slot, GATE_ROWS:, :]
        for t in range(rows // tile):
            here = slice(t * tile, (t + 1) * tile)
            scores = lax.dot_general(
                qpad[here, :], keys, (((1,), (1,)), ((), ())), preferred_element_type=jnp.float32
            )
            pieces = []
            for j in range(rows // lanes):
                s = scores[:, j * lanes : (j + 1) * lanes] + shift[j : j + 1, :]
                if diagonal:
                    place = lax.broadcasted_iota(jnp.int32, s.shape, 0) + t * tile
                    other = lax.broadcasted_iota(jnp.int32, s.shape, 1) + j * lanes
                    s = jnp.where(other <= place, s, -1e30)
                pieces.append(s)
            most = functools.reduce(jnp.maximum, pieces)
            old = top[here, :]
            new = jnp.maximum(old, jnp.max(most, axis=1, keepdims=True))
            shrink = jnp.exp(old - new)
            raised = [jnp.exp(s - new) for s in pieces]
            total[here, :] = total[here, :] * shrink + functools.reduce(jnp.add, raised)
            weights = jnp.concatenate([r.astype(jnp.bfloat16) for r in raised], axis=1)
            summed[here, :] = summed[here, :] * shrink + jnp.dot(
                weights, keys, preferred_element_type=jnp.float32
            )
            top[here, :] = new

    attend(sp, True)

    def earlier(slot):
        @pl.when(slot < sp)
        def _():
            attend(slot, False)

    def slots(step):
        up_from = lax.rem(chip + chips - step, chips)
        down_from = lax.rem(chip + step, chips)
        return up_from, down_from

    def arrive(slot, step, way, part, target, send):
        hop(slot, step, way, part, target).wait_recv()
        if send is True:
            hop(slot, step, way, part, target).start()
        elif send is not False:

            @pl.when(send)
            def _():
                hop(slot, step, way, part, target).start()

    def partner(step, way, slot):
        share(slot, step, way).wait_recv()
        earlier(slot)

    def both(step):
        up_from, down_from = slots(step)
        before_up, before_down = slots(step - 1)
        up_slot, down_slot = up_from * 2 + core, down_from * 2 + core
        for part in range(2):
            arrive(up_slot, step, 0, part, up_sp, step < ups)
        share(up_slot, step, 0).start()
        earlier(up_slot)
        for part in range(2):
            arrive(down_slot, step, 1, part, down_sp, step < downs)
        share(down_slot, step, 1).start()
        earlier(down_slot)
        partner(step - 1, 0, before_up * 2 + 1 - core)

        @pl.when(step == max(1, downs - 2))
        def _():
            for m in range(3):
                ring_forward(y_size, y, weight_copy(m))

        @pl.when(step >= 2)
        def _():
            partner(step - 1, 1, before_down * 2 + 1 - core)

    if downs >= 1:
        lax.fori_loop(1, downs + 1, lambda i, c: (both(i), c)[1], 0)
    last_up, last_down = slots(downs)
    up_from, _ = slots(ups)
    up_slot = up_from * 2 + core
    for part in range(2):
        arrive(up_slot, ups, 0, part, up_sp, False)
    share(up_slot, ups, 0).start()
    earlier(up_slot)
    partner(downs, 0, last_up * 2 + 1 - core)
    if downs >= 1:
        partner(downs, 1, last_down * 2 + 1 - core)
    partner(ups, 0, up_from * 2 + 1 - core)

    def finished(lo):
        here = slice(lo, lo + half)
        whole = jnp.sum(total[here, :], axis=1, keepdims=True)
        return summed[here, :] / whole

    left = pltpu.roll(finished(0), size, 1)
    right = finished(half)
    lane = lax.broadcasted_iota(jnp.int32, left.shape, 1)
    att_all[tp] = jnp.where(lane < size, left, right).astype(jnp.bfloat16)

    def give(d):
        return remote(
            att_all.at[tp],
            att_all.at[tp],
            att_send.at[d],
            att_recv.at[tp],
            tp=lax.rem(tp + d, tp_size),
        )

    def take(d):
        owner = lax.rem(tp + tp_size - d, tp_size)
        return remote(
            att_all.at[owner],
            att_all.at[owner],
            att_send.at[d],
            att_recv.at[owner],
            tp=owner,
        )

    for d in range(1, tp_size):
        give(d).start()
    for d in range(1, tp_size):
        take(d).wait_recv()
    projected = jnp.zeros((half, wide.shape[1]), jnp.float32)
    for j in range(tp_size // 2):
        pair = jnp.concatenate([att_all[2 * j], att_all[2 * j + 1]], axis=1)
        projected += jnp.dot(
            pair, wide[j * 4 * size : (j + 1) * 4 * size, :], preferred_element_type=jnp.float32
        )
    columns = weight_ref.shape[1]
    for part in range(2):
        here = slice(part * half, (part + 1) * half)
        mixed_ref[here, :] = (
            residual_ref[here, :].astype(jnp.float32)
            + projected[:, part * columns : (part + 1) * columns]
        ).astype(jnp.bfloat16)

    for m in range(3):
        if downs < 1:
            ring_forward(y_size, y, weight_copy(m))
        ring_finish(y_size, y, weight_copy(m))
        ring_sent(y_size, y, weight_copy(m))
        locals_w[m].wait()

    if ups >= 1:
        for step in range(ups):
            for part in range(2):
                hop(sp, step, 0, part, up_sp).wait_send()
        for step in range(downs):
            for part in range(2):
                hop(sp, step, 1, part, down_sp).wait_send()
        for step in range(1, ups + 1):
            share(sp, step, 0).wait_send()
        for step in range(1, downs + 1):
            share(sp, step, 1).wait_send()
    share(sp, 0, 0).wait_send()
    for d in range(1, tp_size):
        give(d).wait_send()


def y_of(tp_size):
    return math.isqrt(tp_size)


def attention(
    mesh,
    query_rows,
    key_rows,
    value_rows,
    cum_gates,
    residual,
    output_weight,
    gate_weight,
    up_weight,
    down_weight,
):
    sp_size, tp_size = mesh.shape["sp"], mesh.shape["tp"]
    rows, size = query_rows.shape
    columns = output_weight.shape[1]
    vmem = pl.BlockSpec(memory_space=pltpu.VMEM)
    anywhere = pl.BlockSpec(memory_space=pl.ANY)
    y_size = y_of(tp_size)
    chips = sp_size // 2
    steps = chips // 2 + 1
    return pl.pallas_call(
        functools.partial(attention_kernel, sp_size, tp_size, y_size),
        out_shape=[jax.ShapeDtypeStruct((rows, columns), jnp.bfloat16)]
        + [
            jax.ShapeDtypeStruct((y_size, *w.shape[1:]), jnp.bfloat16)
            for w in (gate_weight, up_weight, down_weight)
        ],
        in_specs=[vmem] * 6 + [anywhere] * 3,
        out_specs=[vmem] + [anywhere] * 3,
        scratch_shapes=[
            pltpu.VMEM((sp_size, GATE_ROWS + rows, 2 * size), jnp.bfloat16),
            pltpu.VMEM((rows, 2 * size), jnp.bfloat16),
            pltpu.VMEM((tp_size * 2 * size, 2 * columns), jnp.bfloat16),
            pltpu.VMEM((rows, 2 * size), jnp.float32),
            pltpu.VMEM((rows, 2 * size), jnp.float32),
            pltpu.VMEM((rows, 2 * size), jnp.float32),
            pltpu.VMEM((tp_size, rows // 2, 2 * size), jnp.bfloat16),
            pltpu.SemaphoreType.DMA((sp_size, 2)),
            pltpu.SemaphoreType.DMA((sp_size,)),
            pltpu.SemaphoreType.DMA((steps, 2, 2)),
            pltpu.SemaphoreType.DMA((steps, 2)),
            pltpu.SemaphoreType.DMA((tp_size,)),
            pltpu.SemaphoreType.DMA((tp_size,)),
            pltpu.SemaphoreType.DMA((3,)),
            pltpu.SemaphoreType.DMA((3, y_size, 2)),
            pltpu.SemaphoreType.DMA((3, 2, 3)),
        ],
        compiler_params=pltpu.CompilerParams(
            collective_id=0, has_side_effects=True, vmem_limit_bytes=40 << 20
        ),
        cost_estimate=pl.CostEstimate(
            flops=4 * rows * rows * sp_size * 2 * size,
            bytes_accessed=1 << 22,
            transcendentals=rows * rows * sp_size,
        ),
    )(
        query_rows,
        key_rows,
        value_rows,
        cum_gates.reshape(4, rows // 4),
        residual,
        output_weight,
        gate_weight,
        up_weight,
        down_weight,
    )


CAP = 64


def expert_kernel(
    sp_size,
    tp_size,
    y_size,
    mixed_ref,
    slot_row,
    slot_col,
    route_ref,
    gain_ref,
    gate_all,
    up_all,
    down_all,
    out_ref,
    outgoing,
    landed,
    tokens,
    normed,
    gate_v,
    up_v,
    down_v,
    hidden,
    produced,
    turned,
    returned,
    load_sem,
    z_send,
    z_recv,
    t_send,
    t_recv,
    h_send,
    h_recv,
    y_send,
    y_recv,
    r_send,
    r_recv,
):
    x_size = tp_size // y_size
    chips = sp_size // 2
    sp = lax.axis_index("sp")
    tp = lax.axis_index("tp")
    y = tp // x_size
    x = tp - y * x_size
    chip = sp // 2
    core = sp - 2 * chip
    rows, columns = mixed_ref.shape
    group = sp_size // y_size
    chunks = 2
    blocks = group // chunks
    height = blocks * CAP
    width = tp_size * columns
    hid = y_size * columns

    barrier = pltpu.get_barrier_semaphore()
    for d in range(1, sp_size):
        pl.semaphore_signal(
            barrier, inc=1, device_id={"sp": lax.rem(sp + d, sp_size)}, device_id_type=MESH
        )
    for d in range(1, tp_size):
        pl.semaphore_signal(
            barrier, inc=1, device_id={"tp": lax.rem(tp + d, tp_size)}, device_id_type=MESH
        )
    loads = []
    for m, (source, target) in enumerate(((gate_all, gate_v), (up_all, up_v), (down_all, down_v))):
        for k in range(y_size):
            loads.append(
                pltpu.make_async_copy(
                    source.at[k],
                    target.at[:, pl.ds(k * columns, columns)],
                    load_sem.at[m, k],
                )
            )
    for load in loads:
        load.start()

    mixed = mixed_ref[...]
    batch = min(4, sp_size)
    first, second = slot_row[0:1, :], slot_row[1:2, :]
    for c in range(sp_size // batch):
        number = lax.broadcasted_iota(jnp.int32, (batch * CAP, rows), 0) + c * batch * CAP
        chosen = jnp.logical_or(number == first, number == second)
        picked = jnp.dot(
            chosen.astype(jnp.float32).astype(jnp.bfloat16),
            mixed,
            preferred_element_type=jnp.float32,
        ).astype(jnp.bfloat16)
        for b in range(batch):
            outgoing[c * batch + b] = picked[b * CAP : (b + 1) * CAP]
    landed[sp] = outgoing[sp]
    pl.semaphore_wait(barrier, sp_size - 1 + tp_size - 1)

    def near(i):
        j = i // 2
        far = (j + 1) // 2
        odd = j - 2 * (j // 2)
        chip_there = lax.rem(chip + chips + (2 * odd - 1) * far, chips)
        other = i - 2 * j
        return chip_there * 2 + core + other * (1 - 2 * core)

    def send_z(i):
        there = near(i)
        return remote(
            outgoing.at[there], landed.at[sp], z_send.at[i], z_recv.at[sp], sp=there
        )

    def take_z(source):
        return remote(outgoing.at[sp], landed.at[source], z_send.at[0], z_recv.at[source], sp=source)

    lax.fori_loop(1, sp_size, lambda i, c: (send_z(i).start(), c)[1], 0)

    def give_t(i, d, source):
        y_there = source // group
        slot = source - y_there * group
        return remote(
            landed.at[source],
            tokens.at[slot, tp],
            t_send.at[i, d],
            t_recv.at[slot],
            tp=y_there * x_size + lax.rem(x + d, x_size),
        )

    def own_t(source):
        slot = source - (source // group) * group
        return pltpu.make_async_copy(landed.at[source], tokens.at[slot, tp], t_recv.at[slot])

    def pass_on(i, source):
        for d in range(1, x_size):
            give_t(i, d, source).start()

        @pl.when(source // group == y)
        def _():
            own_t(source).start()

        @pl.when(source // group != y)
        def _():
            give_t(i, 0, source).start()

    pass_on(0, sp)

    def arrived(i):
        source = near(i)
        take_z(source).wait_recv()
        pass_on(i, source)

    lax.fori_loop(1, sp_size, lambda i, c: (arrived(i), c)[1], 0)

    def h_copy(c):
        def make(owner, k, step, way, index):
            here = hidden.at[
                pl.ds(k * (y_size // 2), y_size // 2), owner, pl.ds(c * height, height), :
            ]
            return remote(
                here,
                here,
                h_send.at[c, way, index],
                h_recv.at[c, owner, k],
                tp=y * x_size + lax.rem(x + step, x_size),
            )

        return make

    for load in loads[: 2 * y_size]:
        load.wait()
    for c in range(chunks):
        for b in range(blocks):
            slot = c * blocks + b
            pltpu.make_async_copy(tokens.at[slot], tokens.at[slot], t_recv.at[slot]).wait()
            squares = jnp.zeros((CAP, columns), jnp.float32)
            for t in range(tp_size):
                wide = tokens[slot, t].astype(jnp.float32)
                squares += wide * wide
            scale = lax.rsqrt(jnp.sum(squares, axis=1, keepdims=True) / width + NORM_EPS)
            for t in range(tp_size):
                wide = tokens[slot, t].astype(jnp.float32)
                normed[slot * CAP : (slot + 1) * CAP, t * columns : (t + 1) * columns] = (
                    wide * scale * gain_ref[t : t + 1, :]
                ).astype(jnp.bfloat16)
        here = slice(c * height, (c + 1) * height)
        tile = min(256, hid)
        for n in range(hid // tile):
            cols = slice(n * tile, (n + 1) * tile)
            gate_input = jnp.dot(normed[here, :], gate_v[:, cols], preferred_element_type=jnp.float32)
            linear_input = jnp.dot(normed[here, :], up_v[:, cols], preferred_element_type=jnp.float32)
            cut = jnp.minimum(gate_input, CLAMP_LIMIT)
            linear = jnp.clip(linear_input, -CLAMP_LIMIT, CLAMP_LIMIT)
            active = (cut / (1.0 + jnp.exp(-SILU_ALPHA * cut)) * (linear + 1.0)).astype(jnp.bfloat16)
            for k in range(tile // columns):
                hidden[n * (tile // columns) + k, x, here, :] = active[
                    :, k * columns : (k + 1) * columns
                ]
        ring_start(x_size, x, h_copy(c))

    def give_y(c, d):
        y_there = lax.rem(y + d, y_size)
        here = pl.ds(c * height, height)
        return remote(
            produced.at[y_there, here, :],
            turned.at[y, here, :],
            y_send.at[c, d],
            y_recv.at[c, y],
            tp=y_there * x_size + x,
        )

    def take_y(c, d):
        source = lax.rem(y + y_size - d, y_size)
        here = pl.ds(c * height, height)
        return source, remote(
            produced.at[source, here, :],
            turned.at[source, here, :],
            y_send.at[c, d],
            y_recv.at[c, source],
            tp=source * x_size + x,
        )

    def send_r(source, slot):
        there = source * group + slot
        return remote(
            turned.at[source, pl.ds(slot * CAP, CAP), :],
            returned.at[sp],
            r_send.at[there],
            r_recv.at[sp],
            sp=there,
        )

    def give_back(source, c):
        for b in range(blocks):
            slot = c * blocks + b
            there = source * group + slot

            @pl.when(there == sp)
            def _():
                returned[sp] = turned[source, slot * CAP : (slot + 1) * CAP, :]

            @pl.when(there != sp)
            def _():
                send_r(source, slot).start()

    for load in loads[2 * y_size :]:
        load.wait()
    for c in range(chunks):
        ring_forward(x_size, x, h_copy(c))
    for c in range(chunks):
        here = slice(c * height, (c + 1) * height)
        ring_finish(x_size, x, h_copy(c))
        made = jnp.zeros((height, hid), jnp.float32)
        for t in range(0, tp_size, 2):
            k, j = t // x_size, t % x_size
            pair = jnp.concatenate([hidden[k, j, here, :], hidden[k, j + 1, here, :]], axis=1)
            made += jnp.dot(
                pair,
                down_v[t * columns : (t + 2) * columns, :],
                preferred_element_type=jnp.float32,
            )
        for k in range(y_size):
            produced[k, here, :] = made[:, k * columns : (k + 1) * columns].astype(jnp.bfloat16)
        for d in range(1, y_size):
            give_y(c, d).start()
        turned[y, here, :] = produced[y, here, :]
        give_back(y, c)
    for c in range(chunks):
        for d in range(1, y_size):
            source, copy = take_y(c, d)
            copy.wait_recv()
            give_back(source, c)

    sums = [jnp.zeros((rows, columns), jnp.float32) for _ in range(2)]
    for c in range(sp_size // batch):
        for b in range(batch):
            e = c * batch + b

            @pl.when(sp != e)
            def _():
                remote(
                    turned.at[0, pl.ds(0, CAP), :],
                    returned.at[e],
                    r_send.at[e],
                    r_recv.at[e],
                    sp=sp,
                ).wait_recv()

        block = jnp.concatenate([returned[c * batch + b] for b in range(batch)], axis=0)
        number = lax.broadcasted_iota(jnp.int32, (rows, batch * CAP), 1) + c * batch * CAP
        for k in range(2):
            chosen = (number == slot_col[:, k : k + 1]).astype(jnp.float32).astype(jnp.bfloat16)
            sums[k] += jnp.dot(chosen, block, preferred_element_type=jnp.float32)
    blended = route_ref[:, 0:1] * sums[0] + route_ref[:, 1:2] * sums[1]
    out_ref[...] = (mixed.astype(jnp.float32) + blended).astype(jnp.bfloat16)

    for i in range(1, sp_size):
        send_z(i).wait_send()
    for i in range(sp_size):
        for d in range(1, x_size):
            give_t(i, d, sp).wait_send()

        @pl.when(near(i) // group != y)
        def _():
            give_t(i, 0, sp).wait_send()

    for c in range(chunks):
        ring_sent(x_size, x, h_copy(c))
        for d in range(1, y_size):
            give_y(c, d).wait_send()
    for e in range(sp_size):

        @pl.when(sp != e)
        def _():
            send_r(e // group, e % group).wait_send()


def experts(mesh, mixed, slot, route_weights, norm_gain, gate_all, up_all, down_all):
    sp_size, tp_size = mesh.shape["sp"], mesh.shape["tp"]
    y_size = y_of(tp_size)
    x_size = tp_size // y_size
    rows, columns = mixed.shape
    group = sp_size // y_size
    depth = gate_all.shape[1]
    hid = y_size * columns
    vmem = pl.BlockSpec(memory_space=pltpu.VMEM)
    anywhere = pl.BlockSpec(memory_space=pl.ANY)
    bf16 = jnp.bfloat16
    dma = pltpu.SemaphoreType.DMA
    return pl.pallas_call(
        functools.partial(expert_kernel, sp_size, tp_size, y_size),
        out_shape=jax.ShapeDtypeStruct((rows, columns), bf16),
        in_specs=[vmem] * 5 + [anywhere] * 3,
        out_specs=vmem,
        scratch_shapes=[
            pltpu.VMEM((sp_size, CAP, columns), bf16),
            pltpu.VMEM((sp_size, CAP, columns), bf16),
            pltpu.VMEM((group, tp_size, CAP, columns), bf16),
            pltpu.VMEM((group * CAP, tp_size * columns), bf16),
            pltpu.VMEM((depth, hid), bf16),
            pltpu.VMEM((depth, hid), bf16),
            pltpu.VMEM((depth, hid), bf16),
            pltpu.VMEM((y_size, x_size, group * CAP, columns), bf16),
            pltpu.VMEM((y_size, group * CAP, columns), bf16),
            pltpu.VMEM((y_size, group * CAP, columns), bf16),
            pltpu.VMEM((sp_size, CAP, columns), bf16),
            dma((3, y_size)),
            dma((sp_size,)),
            dma((sp_size,)),
            dma((sp_size, x_size)),
            dma((group,)),
            dma((2, 2, 3)),
            dma((2, x_size, 2)),
            dma((2, y_size)),
            dma((2, y_size)),
            dma((sp_size,)),
            dma((sp_size,)),
        ],
        compiler_params=pltpu.CompilerParams(
            collective_id=1, has_side_effects=True, vmem_limit_bytes=48 << 20
        ),
        cost_estimate=pl.CostEstimate(
            flops=6 * group * CAP * depth * hid, bytes_accessed=1 << 23, transcendentals=1 << 18
        ),
    )(
        mixed,
        slot.T,
        slot,
        route_weights,
        norm_gain.astype(jnp.float32).reshape(tp_size, columns),
        gate_all,
        up_all,
        down_all,
    )


def slots_of(expert_index, count):
    rows, topk = expert_index.shape
    chosen = expert_index.reshape(rows * topk)
    matches = chosen[:, None] == jnp.arange(count, dtype=jnp.int32)[None, :]
    order = jnp.arange(rows * topk, dtype=jnp.int32)
    before = (order[None, :] < order[:, None]).astype(jnp.bfloat16)
    ahead = jnp.dot(before, matches.astype(jnp.bfloat16), preferred_element_type=jnp.float32)
    rank = jnp.sum(jnp.where(matches, ahead, 0.0), axis=1).astype(jnp.int32)
    return (chosen * CAP + rank).reshape(rows, topk)


def body(
    mesh,
    query_rows,
    key_rows,
    value_rows,
    cum_gates,
    residual,
    output_weight,
    norm_gain,
    expert_index,
    route_weights,
    gate_weight,
    up_weight,
    down_weight,
):
    slot = slots_of(expert_index, mesh.shape["sp"])
    mixed, gate_all, up_all, down_all = attention(
        mesh,
        query_rows,
        key_rows,
        value_rows,
        cum_gates,
        residual,
        output_weight,
        gate_weight,
        up_weight,
        down_weight,
    )
    return experts(mesh, mixed, slot, route_weights, norm_gain, gate_all, up_all, down_all)


def solution(mesh):
    placed = (
        P("sp", "tp"),
        P("sp", "tp"),
        P("sp", "tp"),
        P("sp", "tp"),
        P("sp", "tp"),
        P(None, "tp"),
        P(),
        P("sp", None),
        P("sp", None),
        P("sp", None, "tp"),
        P("sp", None, "tp"),
        P("sp", None, "tp"),
    )
    return jax.shard_map(
        functools.partial(body, mesh),
        mesh=mesh,
        in_specs=placed,
        out_specs=P("sp", "tp"),
        check_vma=False,
    )
```

```python
import functools
import math

import jax
import jax.numpy as jnp
from jax import lax
from jax.experimental import pallas as pl
from jax.experimental.pallas import tpu as pltpu
from jax.sharding import PartitionSpec as P

NORM_EPS = 1e-06
CLAMP_LIMIT = 7.0
SILU_ALPHA = 1.702
MESH = pl.DeviceIdType.MESH
GATE_ROWS = 16


def remote(src, dst, send_sem, recv_sem, **where):
    return pltpu.make_async_remote_copy(
        src_ref=src,
        dst_ref=dst,
        send_sem=send_sem,
        recv_sem=recv_sem,
        device_id=where,
        device_id_type=MESH,
    )


def ring_start(n, place, make):
    if n == 4:
        for k in range(2):
            make(place, k, 1, 0, k).start()
            make(place, 1 - k, 3, 1, k).start()
    elif n == 2:
        for k in range(2):
            make(place, k, 1, 0, k).start()


def ring_forward(n, place, make):
    if n == 4:
        before, after = lax.rem(place + 3, 4), lax.rem(place + 1, 4)
        make(before, 0, 1, 0, 2).wait_recv()
        make(before, 0, 1, 0, 2).start()
        make(after, 1, 3, 1, 2).wait_recv()
        make(after, 1, 3, 1, 2).start()


def ring_finish(n, place, make):
    if n == 4:
        make(lax.rem(place + 3, 4), 1, 1, 0, 0).wait_recv()
        make(lax.rem(place + 1, 4), 0, 1, 0, 0).wait_recv()
        for k in range(2):
            make(lax.rem(place + 2, 4), k, 1, 0, 0).wait_recv()
    elif n == 2:
        for k in range(2):
            make(1 - place, k, 1, 0, 0).wait_recv()


def ring_sent(n, place, make):
    if n == 4:
        for k in range(3):
            half = k if k < 2 else 0
            make(place, half, 1, 0, k).wait_send()
            make(place, 1 - half, 3, 1, k).wait_send()
    elif n == 2:
        for k in range(2):
            make(place, k, 1, 0, k).wait_send()


def layer_kernel(
    sp_size,
    tp_size,
    y_size,
    q_ref,
    k_ref,
    v_ref,
    gate_ref,
    residual_ref,
    weight_ref,
    gate_w,
    up_w,
    down_w,
    slot_row,
    slot_col,
    route_ref,
    gain_ref,
    out_ref,
    q_v,
    k_v,
    v_v,
    gate_rows,
    residual_v,
    weight_v,
    mixed_v,
    kv_all,
    qpad,
    wide,
    top,
    total,
    summed,
    att_all,
    outgoing,
    landed,
    tokens,
    normed,
    gate_v,
    up_v,
    down_v,
    hidden,
    produced,
    turned,
    returned,
    in_sem,
    kv_recv,
    own_recv,
    ring_send,
    pair_send,
    att_recv,
    att_send,
    own_w,
    w_recv,
    w_send,
    z_send,
    z_recv,
    t_send,
    t_recv,
    h_send,
    h_recv,
    y_send,
    y_recv,
    r_send,
    r_recv,
):
    chips = sp_size // 2
    ups = chips // 2
    downs = chips - 1 - ups
    sp = lax.axis_index("sp")
    tp = lax.axis_index("tp")
    chip = sp // 2
    core = sp - 2 * chip
    size, rows = q_ref.shape
    half = rows // 2
    x_size = tp_size // y_size
    y = tp // x_size
    x = tp - y * x_size
    quarter = rows // 4
    starts = [0] + [GATE_ROWS + k * quarter for k in range(1, 4)]
    lengths = [GATE_ROWS + quarter] + [quarter] * 3
    parts = range(4)
    up_sp = lax.rem(chip + 1, chips) * 2 + core
    down_sp = lax.rem(chip + chips - 1, chips) * 2 + core
    pair_sp = chip * 2 + 1 - core

    barrier = pltpu.get_barrier_semaphore()
    for d in range(1, sp_size):
        pl.semaphore_signal(
            barrier, inc=1, device_id={"sp": lax.rem(sp + d, sp_size)}, device_id_type=MESH
        )
    for d in range(1, tp_size):
        pl.semaphore_signal(
            barrier, inc=1, device_id={"tp": lax.rem(tp + d, tp_size)}, device_id_type=MESH
        )

    inputs = [
        pltpu.make_async_copy(source, target, in_sem.at[k])
        for k, (source, target) in enumerate(
            (
                (q_ref, q_v),
                (k_ref, k_v),
                (v_ref, v_v),
                (gate_ref, gate_rows),
                (residual_ref, residual_v),
                (weight_ref, weight_v),
            )
        )
    ]
    for load in inputs:
        load.start()
    for load in inputs[:4]:
        load.wait()

    gates = gate_rows[...]
    high = gates.astype(jnp.bfloat16)
    rest = gates - high.astype(jnp.float32)
    middle = rest.astype(jnp.bfloat16)
    low = (rest - middle.astype(jnp.float32)).astype(jnp.bfloat16)
    kv_all[sp, 0:GATE_ROWS, :] = jnp.concatenate(
        [
            high.astype(jnp.float32),
            middle.astype(jnp.float32),
            low.astype(jnp.float32),
            jnp.zeros_like(gates),
        ],
        axis=0,
    ).astype(jnp.bfloat16)
    both_kv = jnp.concatenate([k_v[...], v_v[...]], axis=0).astype(jnp.float32)
    kv_all[sp, GATE_ROWS:, :] = both_kv.T.astype(jnp.bfloat16)
    qs = q_v[...].astype(jnp.float32) * (size**-0.5)
    qpad[...] = jnp.concatenate([qs, jnp.zeros_like(qs)], axis=0).T.astype(jnp.bfloat16)
    first_gate = gates[0:1, 0:1]

    pl.semaphore_wait(barrier, sp_size - 1 + tp_size - 1)

    def piece(slot, part):
        return kv_all.at[slot, pl.ds(starts[part], lengths[part]), :]

    def hop(slot, step, way, part, target):
        return remote(
            piece(slot, part),
            piece(slot, part),
            ring_send.at[step, way, part],
            kv_recv.at[slot, part],
            sp=target,
        )

    def share(slot, step, way):
        return remote(
            kv_all.at[slot],
            kv_all.at[slot],
            pair_send.at[step, way],
            own_recv.at[slot],
            sp=pair_sp,
        )

    matrices = ((gate_w, gate_v), (up_w, up_v), (down_w, down_v))
    depth = gate_w.shape[1]
    columns = weight_ref.shape[1]

    def lanes_of(owner):
        return pl.ds(pl.multiple_of(owner * columns, columns), columns)

    def weight_copy(m):
        own, every = matrices[m]

        def make(owner, k, step, way, index):
            here = every.at[pl.ds(k * (depth // 2), depth // 2), lanes_of(owner)]
            mine = own.at[0, pl.ds(k * (depth // 2), depth // 2), :]
            return remote(
                mine if index < 2 else here,
                here,
                w_send.at[m, way, index],
                w_recv.at[m, owner, k],
                tp=lax.rem(y + step, y_size) * x_size + x,
            )

        return make

    def own_weight(m):
        own, every = matrices[m]
        return pltpu.make_async_copy(own.at[0], every.at[:, lanes_of(y)], own_w.at[m])

    def weight_start(m):
        ring_start(y_size, y, weight_copy(m))
        own_weight(m).start()

    def weight_ready(m):
        ring_finish(y_size, y, weight_copy(m))
        own_weight(m).wait()

    if ups >= 1:
        for part in parts:
            hop(sp, 0, 0, part, up_sp).start()
            if downs >= 1:
                hop(sp, 0, 1, part, down_sp).start()
    share(sp, 0, 0).start()
    for m in range(2):
        weight_start(m)
    for load in inputs[4:]:
        load.wait()

    wide[...] = jnp.zeros_like(wide)
    for h in range(tp_size):
        w = weight_v[h * size : (h + 1) * size, :]
        wide[h * 2 * size : h * 2 * size + size, 0 : w.shape[1]] = w
        wide[h * 2 * size + size : (h + 1) * 2 * size, w.shape[1] :] = w

    top[...] = jnp.full_like(top, -1e30)
    total[...] = jnp.zeros_like(total)
    summed[...] = jnp.zeros_like(summed)
    tile = min(128, rows)
    lanes = 128

    def attend(slot, diagonal):
        parts = kv_all[slot, 0:GATE_ROWS, :].astype(jnp.float32)
        n4 = GATE_ROWS // 4
        key_gates = parts[0:n4] + parts[n4 : 2 * n4] + parts[2 * n4 : 3 * n4]
        shift = first_gate - key_gates
        keys = kv_all[slot, GATE_ROWS:, :]
        for t in range(rows // tile):
            here = slice(t * tile, (t + 1) * tile)
            scores = lax.dot_general(
                qpad[here, :], keys, (((1,), (1,)), ((), ())), preferred_element_type=jnp.float32
            )
            pieces = []
            for j in range(rows // lanes):
                s = scores[:, j * lanes : (j + 1) * lanes] + shift[j : j + 1, :]
                if diagonal:
                    place = lax.broadcasted_iota(jnp.int32, s.shape, 0) + t * tile
                    other = lax.broadcasted_iota(jnp.int32, s.shape, 1) + j * lanes
                    s = jnp.where(other <= place, s, -1e30)
                pieces.append(s)
            most = functools.reduce(jnp.maximum, pieces)
            old = top[here, :]
            new = jnp.maximum(old, jnp.max(most, axis=1, keepdims=True))
            shrink = jnp.exp(old - new)
            raised = [jnp.exp(s - new) for s in pieces]
            total[here, :] = total[here, :] * shrink + functools.reduce(jnp.add, raised)
            weights = jnp.concatenate([r.astype(jnp.bfloat16) for r in raised], axis=1)
            summed[here, :] = summed[here, :] * shrink + jnp.dot(
                weights, keys, preferred_element_type=jnp.float32
            )
            top[here, :] = new

    attend(sp, True)

    def earlier(slot):
        @pl.when(slot < sp)
        def _():
            attend(slot, False)

    def slots(step):
        up_from = lax.rem(chip + chips - step, chips)
        down_from = lax.rem(chip + step, chips)
        return up_from, down_from

    def arrive(slot, step, way, part, target, send):
        hop(slot, step, way, part, target).wait_recv()
        if send is True:
            hop(slot, step, way, part, target).start()
        elif send is not False:

            @pl.when(send)
            def _():
                hop(slot, step, way, part, target).start()

    def partner(step, way, slot):
        share(slot, step, way).wait_recv()
        earlier(slot)

    def both(step):
        up_from, down_from = slots(step)
        before_up, before_down = slots(step - 1)
        up_slot, down_slot = up_from * 2 + core, down_from * 2 + core

        def pieces(these):
            for part in these:
                arrive(up_slot, step, 0, part, up_sp, step < ups)
                arrive(down_slot, step, 1, part, down_sp, step < downs)

        pieces(parts[:2])
        partner(step - 1, 0, before_up * 2 + 1 - core)

        @pl.when(step >= 2)
        def _():
            partner(step - 1, 1, before_down * 2 + 1 - core)

        pieces(parts[2:])
        share(up_slot, step, 0).start()
        share(down_slot, step, 1).start()
        for m in range(2):

            @pl.when(step == max(1, downs - 3 * (1 - m)))
            def _():
                ring_forward(y_size, y, weight_copy(m))

        earlier(up_slot)
        earlier(down_slot)

    if downs >= 1:
        lax.fori_loop(1, downs + 1, lambda i, c: (both(i), c)[1], 0)
    else:
        for m in range(2):
            ring_forward(y_size, y, weight_copy(m))
    last_up, last_down = slots(downs)
    up_from, _ = slots(ups)
    up_slot = up_from * 2 + core
    for part in parts:
        arrive(up_slot, ups, 0, part, up_sp, False)
    share(up_slot, ups, 0).start()
    partner(downs, 0, last_up * 2 + 1 - core)
    if downs >= 1:
        partner(downs, 1, last_down * 2 + 1 - core)
    earlier(up_slot)
    partner(ups, 0, up_from * 2 + 1 - core)

    def finished(lo):
        here = slice(lo, lo + half)
        whole = jnp.sum(total[here, :], axis=1, keepdims=True)
        return summed[here, :] / whole

    left = pltpu.roll(finished(0), size, 1)
    right = finished(half)
    lane = lax.broadcasted_iota(jnp.int32, left.shape, 1)
    att_all[tp] = jnp.where(lane < size, left, right).astype(jnp.bfloat16)

    def give(d):
        return remote(
            att_all.at[tp],
            att_all.at[tp],
            att_send.at[d],
            att_recv.at[tp],
            tp=lax.rem(tp + d, tp_size),
        )

    def take(d):
        owner = lax.rem(tp + tp_size - d, tp_size)
        return remote(
            att_all.at[owner],
            att_all.at[owner],
            att_send.at[d],
            att_recv.at[owner],
            tp=owner,
        )

    for d in range(1, tp_size):
        give(d).start()
    for d in range(1, tp_size):
        take(d).wait_recv()
    weight_start(2)
    projected = jnp.zeros((half, wide.shape[1]), jnp.float32)
    for j in range(tp_size // 2):
        pair = jnp.concatenate([att_all[2 * j], att_all[2 * j + 1]], axis=1)
        projected += jnp.dot(
            pair, wide[j * 4 * size : (j + 1) * 4 * size, :], preferred_element_type=jnp.float32
        )
    for part in range(2):
        here = slice(part * half, (part + 1) * half)
        mixed_v[here, :] = (
            residual_v[here, :].astype(jnp.float32)
            + projected[:, part * columns : (part + 1) * columns]
        ).astype(jnp.bfloat16)


    group = sp_size // y_size
    chunks = 2
    share_rows = 2 * 2 * rows // sp_size // chunks
    height = group * share_rows
    width = tp_size * columns
    hid = y_size * columns
    batch = min(sp_size, max(1, 256 // share_rows))
    span = batch * share_rows

    mixed = mixed_v[...]
    first, second = slot_row[0:1, :], slot_row[1:2, :]

    def near(i):
        j = i // 2
        far = (j + 1) // 2
        odd = j - 2 * (j // 2)
        chip_there = lax.rem(chip + chips + (2 * odd - 1) * far, chips)
        other = i - 2 * j
        return chip_there * 2 + core + other * (1 - 2 * core)

    def send_z(c, i):
        there = near(i)
        return remote(
            outgoing.at[c, there], landed.at[c, sp], z_send.at[c, i], z_recv.at[c, sp], sp=there
        )

    def take_z(c, source):
        return remote(
            outgoing.at[c, sp],
            landed.at[c, source],
            z_send.at[c, 0],
            z_recv.at[c, source],
            sp=source,
        )

    for c in range(chunks):
        for n in range(sp_size // batch):
            start = c * sp_size * share_rows + n * span
            number = lax.broadcasted_iota(jnp.int32, (span, rows), 0) + start
            chosen = jnp.logical_or(number == first, number == second)
            picked = jnp.dot(
                chosen.astype(jnp.float32).astype(jnp.bfloat16),
                mixed,
                preferred_element_type=jnp.float32,
            ).astype(jnp.bfloat16)
            for k in range(batch):
                outgoing[c, n * batch + k] = picked[k * share_rows : (k + 1) * share_rows]
        landed[c, sp] = outgoing[c, sp]
        lax.fori_loop(1, sp_size, lambda i, s: (send_z(c, i).start(), s)[1], 0)

    def give_t(c, i, d, source):
        y_there = source // group
        slot = source - y_there * group
        return remote(
            landed.at[c, source],
            tokens.at[c, slot, tp],
            t_send.at[c, i, d],
            t_recv.at[c],
            tp=y_there * x_size + lax.rem(x + d, x_size),
        )

    def own_t(c, source):
        slot = source - (source // group) * group
        return pltpu.make_async_copy(landed.at[c, source], tokens.at[c, slot, tp], t_recv.at[c])

    def pass_on(c, i, source):
        for d in range(1, x_size):
            give_t(c, i, d, source).start()

        @pl.when(source // group == y)
        def _():
            own_t(c, source).start()

        @pl.when(source // group != y)
        def _():
            give_t(c, i, 0, source).start()

    def arrived(c, i):
        source = near(i)
        take_z(c, source).wait_recv()
        pass_on(c, i, source)

    for c in range(chunks):
        pass_on(c, 0, sp)
        lax.fori_loop(1, sp_size, lambda i, s: (arrived(c, i), s)[1], 0)
        if c == 0:
            ring_forward(y_size, y, weight_copy(2))

    def h_copy(c):
        def make(owner, k, step, way, index):
            here = hidden.at[c, pl.ds(k * (y_size // 2), y_size // 2), owner]
            return remote(
                here,
                here,
                h_send.at[c, way, index],
                h_recv.at[c, owner, k],
                tp=y * x_size + lax.rem(x + step, x_size),
            )

        return make

    for m in range(2):
        weight_ready(m)
    for c in range(chunks):
        pltpu.make_async_copy(tokens.at[c], tokens.at[c], t_recv.at[c]).wait()
        for slot in range(group):
            squares = jnp.zeros((share_rows, columns), jnp.float32)
            for t in range(tp_size):
                piece_t = tokens[c, slot, t].astype(jnp.float32)
                squares += piece_t * piece_t
            scale = lax.rsqrt(jnp.sum(squares, axis=1, keepdims=True) / width + NORM_EPS)
            for t in range(tp_size):
                piece_t = tokens[c, slot, t].astype(jnp.float32)
                normed[
                    slot * share_rows : (slot + 1) * share_rows, t * columns : (t + 1) * columns
                ] = (piece_t * scale * gain_ref[t : t + 1, :]).astype(jnp.bfloat16)
        tile = min(256, hid)
        for n in range(hid // tile):
            cols = slice(n * tile, (n + 1) * tile)
            gate_input = jnp.dot(normed[...], gate_v[:, cols], preferred_element_type=jnp.float32)
            linear_input = jnp.dot(normed[...], up_v[:, cols], preferred_element_type=jnp.float32)
            cut = jnp.minimum(gate_input, CLAMP_LIMIT)
            linear = jnp.clip(linear_input, -CLAMP_LIMIT, CLAMP_LIMIT)
            active = (cut / (1.0 + jnp.exp(-SILU_ALPHA * cut)) * (linear + 1.0)).astype(jnp.bfloat16)
            for k in range(tile // columns):
                hidden[c, n * (tile // columns) + k, x] = active[
                    :, k * columns : (k + 1) * columns
                ]
        ring_start(x_size, x, h_copy(c))

    def give_y(c, d):
        y_there = lax.rem(y + d, y_size)
        return remote(
            produced.at[c, y_there],
            turned.at[c, y],
            y_send.at[c, d],
            y_recv.at[c, y],
            tp=y_there * x_size + x,
        )

    def take_y(c, d):
        source = lax.rem(y + y_size - d, y_size)
        return source, remote(
            produced.at[c, source],
            turned.at[c, source],
            y_send.at[c, d],
            y_recv.at[c, source],
            tp=source * x_size + x,
        )

    def send_r(c, source, slot):
        there = source * group + slot
        return remote(
            turned.at[c, source, pl.ds(slot * share_rows, share_rows), :],
            returned.at[c, sp],
            r_send.at[c, there],
            r_recv.at[c, sp],
            sp=there,
        )

    def give_back(c, source):
        for slot in range(group):
            there = source * group + slot

            @pl.when(there == sp)
            def _():
                returned[c, sp] = turned[
                    c, source, slot * share_rows : (slot + 1) * share_rows, :
                ]

            @pl.when(there != sp)
            def _():
                send_r(c, source, slot).start()

    for c in range(chunks):
        ring_forward(x_size, x, h_copy(c))
    weight_ready(2)
    for c in range(chunks):
        ring_finish(x_size, x, h_copy(c))
        made = jnp.zeros((height, hid), jnp.float32)
        for t in range(0, tp_size, 2):
            k, j = t // x_size, t % x_size
            pair = jnp.concatenate([hidden[c, k, j], hidden[c, k, j + 1]], axis=1)
            made += jnp.dot(
                pair,
                down_v[t * columns : (t + 2) * columns, :],
                preferred_element_type=jnp.float32,
            )
        for k in range(y_size):
            produced[c, k] = made[:, k * columns : (k + 1) * columns].astype(jnp.bfloat16)
        for d in range(1, y_size):
            give_y(c, d).start()
        turned[c, y] = produced[c, y]
        give_back(c, y)
    for c in range(chunks):
        for d in range(1, y_size):
            source, copy = take_y(c, d)
            copy.wait_recv()
            give_back(c, source)

    sums = [jnp.zeros((rows, columns), jnp.float32) for _ in range(2)]
    for c in range(chunks):
        for n in range(sp_size // batch):
            for k in range(batch):
                e = n * batch + k

                @pl.when(sp != e)
                def _():
                    remote(
                        turned.at[c, 0, pl.ds(0, share_rows), :],
                        returned.at[c, e],
                        r_send.at[c, e],
                        r_recv.at[c, e],
                        sp=sp,
                    ).wait_recv()

            block = jnp.concatenate([returned[c, n * batch + k] for k in range(batch)], axis=0)
            start = c * sp_size * share_rows + n * span
            number = lax.broadcasted_iota(jnp.int32, (rows, span), 1) + start
            for k in range(2):
                chosen = (number == slot_col[:, k : k + 1]).astype(jnp.float32).astype(jnp.bfloat16)
                sums[k] += jnp.dot(chosen, block, preferred_element_type=jnp.float32)
    blended = route_ref[:, 0:1] * sums[0] + route_ref[:, 1:2] * sums[1]
    out_ref[...] = (mixed.astype(jnp.float32) + blended).astype(jnp.bfloat16)

    if ups >= 1:
        for step in range(ups):
            for part in parts:
                hop(sp, step, 0, part, up_sp).wait_send()
        for step in range(downs):
            for part in parts:
                hop(sp, step, 1, part, down_sp).wait_send()
        for step in range(1, ups + 1):
            share(sp, step, 0).wait_send()
        for step in range(1, downs + 1):
            share(sp, step, 1).wait_send()
    share(sp, 0, 0).wait_send()
    for d in range(1, tp_size):
        give(d).wait_send()


    for m in range(3):
        ring_sent(y_size, y, weight_copy(m))
    for c in range(chunks):
        for i in range(1, sp_size):
            send_z(c, i).wait_send()
        for i in range(sp_size):
            for d in range(1, x_size):
                give_t(c, i, d, sp).wait_send()

            @pl.when(near(i) // group != y)
            def _():
                give_t(c, i, 0, sp).wait_send()

        ring_sent(x_size, x, h_copy(c))
        for d in range(1, y_size):
            give_y(c, d).wait_send()
        for e in range(sp_size):

            @pl.when(sp != e)
            def _():
                send_r(c, e // group, e % group).wait_send()


def y_of(tp_size):
    return math.isqrt(tp_size)


def layer(
    mesh,
    query_rows,
    key_rows,
    value_rows,
    cum_gates,
    residual,
    output_weight,
    norm_gain,
    slot,
    route_weights,
    gate_weight,
    up_weight,
    down_weight,
):
    sp_size, tp_size = mesh.shape["sp"], mesh.shape["tp"]
    y_size = y_of(tp_size)
    x_size = tp_size // y_size
    rows, size = query_rows.shape
    columns = output_weight.shape[1]
    group = sp_size // y_size
    depth = gate_weight.shape[1]
    hid = y_size * columns
    part = 2 * rows // sp_size
    height = group * part
    steps = sp_size // 4 + 1
    bf16, f32 = jnp.bfloat16, jnp.float32
    vmem = pl.BlockSpec(memory_space=pltpu.VMEM)
    anywhere = pl.BlockSpec(memory_space=pl.ANY)
    dma = pltpu.SemaphoreType.DMA
    gates = cum_gates.reshape(4, rows // 4)
    return pl.pallas_call(
        functools.partial(layer_kernel, sp_size, tp_size, y_size),
        out_shape=jax.ShapeDtypeStruct((rows, columns), bf16),
        in_specs=[anywhere] * 9 + [vmem] * 4,
        out_specs=vmem,
        scratch_shapes=[
            pltpu.VMEM((size, rows), bf16),
            pltpu.VMEM((size, rows), bf16),
            pltpu.VMEM((size, rows), bf16),
            pltpu.VMEM(gates.shape, f32),
            pltpu.VMEM(residual.shape, bf16),
            pltpu.VMEM(output_weight.shape, bf16),
            pltpu.VMEM((rows, columns), bf16),
            pltpu.VMEM((sp_size, GATE_ROWS + rows, 2 * size), bf16),
            pltpu.VMEM((rows, 2 * size), bf16),
            pltpu.VMEM((tp_size * 2 * size, 2 * columns), bf16),
            pltpu.VMEM((rows, 2 * size), f32),
            pltpu.VMEM((rows, 2 * size), f32),
            pltpu.VMEM((rows, 2 * size), f32),
            pltpu.VMEM((tp_size, rows // 2, 2 * size), bf16),
            pltpu.VMEM((2, sp_size, part, columns), bf16),
            pltpu.VMEM((2, sp_size, part, columns), bf16),
            pltpu.VMEM((2, group, tp_size, part, columns), bf16),
            pltpu.VMEM((height, tp_size * columns), bf16),
            pltpu.VMEM((depth, hid), bf16),
            pltpu.VMEM((depth, hid), bf16),
            pltpu.VMEM((depth, hid), bf16),
            pltpu.VMEM((2, y_size, x_size, height, columns), bf16),
            pltpu.VMEM((2, y_size, height, columns), bf16),
            pltpu.VMEM((2, y_size, height, columns), bf16),
            pltpu.VMEM((2, sp_size, part, columns), bf16),
            dma((6,)),
            dma((sp_size, 4)),
            dma((sp_size,)),
            dma((steps, 2, 4)),
            dma((steps, 2)),
            dma((tp_size,)),
            dma((tp_size,)),
            dma((3,)),
            dma((3, y_size, 2)),
            dma((3, 2, 3)),
            dma((2, sp_size)),
            dma((2, sp_size)),
            dma((2, sp_size, x_size)),
            dma((2,)),
            dma((2, 2, 3)),
            dma((2, x_size, 2)),
            dma((2, y_size)),
            dma((2, y_size)),
            dma((2, sp_size)),
            dma((2, sp_size)),
        ],
        compiler_params=pltpu.CompilerParams(
            collective_id=0, has_side_effects=True, vmem_limit_bytes=60 << 20
        ),
    )(
        query_rows.T,
        key_rows.T,
        value_rows.T,
        gates,
        residual,
        output_weight,
        gate_weight,
        up_weight,
        down_weight,
        slot.T,
        slot,
        route_weights,
        norm_gain.astype(f32).reshape(tp_size, columns),
    )


def slots_of(expert_index, count):
    rows, topk = expert_index.shape
    chosen = expert_index.reshape(rows * topk)
    matches = chosen[:, None] == jnp.arange(count, dtype=jnp.int32)[None, :]
    order = jnp.arange(rows * topk, dtype=jnp.int32)
    before = (order[None, :] < order[:, None]).astype(jnp.bfloat16)
    ahead = jnp.dot(before, matches.astype(jnp.bfloat16), preferred_element_type=jnp.float32)
    rank = jnp.sum(jnp.where(matches, ahead, 0.0), axis=1).astype(jnp.int32)
    part = rows * topk // count
    half = rank // part
    return (half * count * part + chosen * part + rank - half * part).reshape(rows, topk)


def body(
    mesh,
    query_rows,
    key_rows,
    value_rows,
    cum_gates,
    residual,
    output_weight,
    norm_gain,
    expert_index,
    route_weights,
    gate_weight,
    up_weight,
    down_weight,
):
    slot = slots_of(expert_index, mesh.shape["sp"])
    return layer(
        mesh,
        query_rows,
        key_rows,
        value_rows,
        cum_gates,
        residual,
        output_weight,
        norm_gain,
        slot,
        route_weights,
        gate_weight,
        up_weight,
        down_weight,
    )


def solution(mesh):
    placed = (
        P("sp", "tp"),
        P("sp", "tp"),
        P("sp", "tp"),
        P("sp", "tp"),
        P("sp", "tp"),
        P(None, "tp"),
        P(),
        P("sp", None),
        P("sp", None),
        P("sp", None, "tp"),
        P("sp", None, "tp"),
        P("sp", None, "tp"),
    )
    return jax.shard_map(
        functools.partial(body, mesh),
        mesh=mesh,
        in_specs=placed,
        out_specs=P("sp", "tp"),
        check_vma=False,
    )
```

```python
import functools
import math

import jax
import jax.numpy as jnp
from jax import lax
from jax.experimental import pallas as pl
from jax.experimental.pallas import tpu as pltpu
from jax.sharding import PartitionSpec as P

NORM_EPS = 1e-06
CLAMP_LIMIT = 7.0
SILU_ALPHA = 1.702
MESH = pl.DeviceIdType.MESH
GATE_ROWS = 16


def remote(src, dst, send_sem, recv_sem, **where):
    return pltpu.make_async_remote_copy(
        src_ref=src,
        dst_ref=dst,
        send_sem=send_sem,
        recv_sem=recv_sem,
        device_id=where,
        device_id_type=MESH,
    )


def ring_start(n, place, make):
    if n == 4:
        for k in range(2):
            make(place, k, 1, 0, k).start()
            make(place, 1 - k, 3, 1, k).start()
    elif n == 2:
        for k in range(2):
            make(place, k, 1, 0, k).start()


def ring_forward(n, place, make):
    if n == 4:
        before, after = lax.rem(place + 3, 4), lax.rem(place + 1, 4)
        make(before, 0, 1, 0, 2).wait_recv()
        make(before, 0, 1, 0, 2).start()
        make(after, 1, 3, 1, 2).wait_recv()
        make(after, 1, 3, 1, 2).start()


def ring_finish(n, place, make):
    if n == 4:
        make(lax.rem(place + 3, 4), 1, 1, 0, 0).wait_recv()
        make(lax.rem(place + 1, 4), 0, 1, 0, 0).wait_recv()
        for k in range(2):
            make(lax.rem(place + 2, 4), k, 1, 0, 0).wait_recv()
    elif n == 2:
        for k in range(2):
            make(1 - place, k, 1, 0, 0).wait_recv()


def ring_sent(n, place, make):
    if n == 4:
        for k in range(3):
            half = k if k < 2 else 0
            make(place, half, 1, 0, k).wait_send()
            make(place, 1 - half, 3, 1, k).wait_send()
    elif n == 2:
        for k in range(2):
            make(place, k, 1, 0, k).wait_send()


def layer_kernel(
    sp_size,
    tp_size,
    y_size,
    q_ref,
    k_ref,
    v_ref,
    gate_ref,
    residual_ref,
    weight_ref,
    gate_w,
    up_w,
    down_w,
    slot_row,
    slot_col,
    route_ref,
    gain_ref,
    out_ref,
    q_v,
    k_v,
    v_v,
    gate_rows,
    residual_v,
    weight_v,
    mixed_v,
    kv_all,
    qpad,
    wide,
    top,
    total,
    summed,
    att_all,
    outgoing,
    landed,
    tokens,
    normed,
    gate_v,
    up_v,
    down_v,
    hidden,
    produced,
    turned,
    returned,
    in_sem,
    kv_recv,
    own_recv,
    ring_send,
    pair_send,
    att_recv,
    att_send,
    own_w,
    w_recv,
    w_send,
    z_send,
    z_recv,
    t_send,
    t_recv,
    h_send,
    h_recv,
    y_send,
    y_recv,
    r_send,
    r_recv,
):
    chips = sp_size // 2
    ups = chips // 2
    downs = chips - 1 - ups
    sp = lax.axis_index("sp")
    tp = lax.axis_index("tp")
    chip = sp // 2
    core = sp - 2 * chip
    size, rows = q_ref.shape
    half = rows // 2
    x_size = tp_size // y_size
    y = tp // x_size
    x = tp - y * x_size
    quarter = rows // 4
    starts = [0] + [GATE_ROWS + k * quarter for k in range(1, 4)]
    lengths = [GATE_ROWS + quarter] + [quarter] * 3
    parts = range(4)
    up_sp = lax.rem(chip + 1, chips) * 2 + core
    down_sp = lax.rem(chip + chips - 1, chips) * 2 + core
    pair_sp = chip * 2 + 1 - core

    barrier = pltpu.get_barrier_semaphore()
    for target in (up_sp, down_sp, pair_sp):
        pl.semaphore_signal(barrier, inc=1, device_id={"sp": target}, device_id_type=MESH)
    for d in range(1, tp_size):
        pl.semaphore_signal(
            barrier, inc=1, device_id={"tp": lax.rem(tp + d, tp_size)}, device_id_type=MESH
        )

    inputs = [
        pltpu.make_async_copy(source, target, in_sem.at[k])
        for k, (source, target) in enumerate(
            (
                (q_ref, q_v),
                (k_ref, k_v),
                (v_ref, v_v),
                (gate_ref, gate_rows),
                (residual_ref, residual_v),
                (weight_ref, weight_v),
            )
        )
    ]
    for load in inputs:
        load.start()
    for load in inputs[:4]:
        load.wait()

    gates = gate_rows[...]
    high = gates.astype(jnp.bfloat16)
    rest = gates - high.astype(jnp.float32)
    middle = rest.astype(jnp.bfloat16)
    low = (rest - middle.astype(jnp.float32)).astype(jnp.bfloat16)
    kv_all[sp, 0:GATE_ROWS, :] = jnp.concatenate(
        [
            high.astype(jnp.float32),
            middle.astype(jnp.float32),
            low.astype(jnp.float32),
            jnp.zeros_like(gates),
        ],
        axis=0,
    ).astype(jnp.bfloat16)
    both_kv = jnp.concatenate([k_v[...], v_v[...]], axis=0).astype(jnp.float32)
    kv_all[sp, GATE_ROWS:, :] = both_kv.T.astype(jnp.bfloat16)
    qs = q_v[...].astype(jnp.float32) * (size**-0.5)
    qpad[...] = jnp.concatenate([qs, jnp.zeros_like(qs)], axis=0).T.astype(jnp.bfloat16)
    first_gate = gates[0:1, 0:1]

    pl.semaphore_wait(barrier, 3 + tp_size - 1)

    def piece(slot, part):
        return kv_all.at[slot, pl.ds(starts[part], lengths[part]), :]

    def hop(slot, step, way, part, target):
        return remote(
            piece(slot, part),
            piece(slot, part),
            ring_send.at[step, way, part],
            kv_recv.at[slot, part],
            sp=target,
        )

    def share(slot, step, way):
        return remote(
            kv_all.at[slot],
            kv_all.at[slot],
            pair_send.at[step, way],
            own_recv.at[slot],
            sp=pair_sp,
        )

    matrices = ((gate_w, gate_v), (up_w, up_v), (down_w, down_v))
    depth = gate_w.shape[1]
    columns = weight_ref.shape[1]

    def lanes_of(owner):
        return pl.ds(pl.multiple_of(owner * columns, columns), columns)

    def weight_copy(m):
        own, every = matrices[m]

        def make(owner, k, step, way, index):
            here = every.at[pl.ds(k * (depth // 2), depth // 2), lanes_of(owner)]
            mine = own.at[0, pl.ds(k * (depth // 2), depth // 2), :]
            return remote(
                mine if index < 2 else here,
                here,
                w_send.at[m, way, index],
                w_recv.at[m, owner, k],
                tp=lax.rem(y + step, y_size) * x_size + x,
            )

        return make

    def own_weight(m):
        own, every = matrices[m]
        return pltpu.make_async_copy(own.at[0], every.at[:, lanes_of(y)], own_w.at[m])

    def weight_start(m):
        ring_start(y_size, y, weight_copy(m))
        own_weight(m).start()

    def weight_ready(m):
        ring_finish(y_size, y, weight_copy(m))
        own_weight(m).wait()

    if ups >= 1:
        for part in parts:
            hop(sp, 0, 0, part, up_sp).start()
            if downs >= 1:
                hop(sp, 0, 1, part, down_sp).start()
    share(sp, 0, 0).start()
    for m in range(2):
        weight_start(m)
    for load in inputs[4:]:
        load.wait()

    wide[...] = jnp.zeros_like(wide)
    for h in range(tp_size):
        w = weight_v[h * size : (h + 1) * size, :]
        wide[h * 2 * size : h * 2 * size + size, 0 : w.shape[1]] = w
        wide[h * 2 * size + size : (h + 1) * 2 * size, w.shape[1] :] = w

    top[...] = jnp.full_like(top, -1e30)
    total[...] = jnp.zeros_like(total)
    summed[...] = jnp.zeros_like(summed)
    tile = rows
    lanes = 128

    def attend(slot, diagonal):
        parts = kv_all[slot, 0:GATE_ROWS, :].astype(jnp.float32)
        n4 = GATE_ROWS // 4
        key_gates = parts[0:n4] + parts[n4 : 2 * n4] + parts[2 * n4 : 3 * n4]
        shift = first_gate - key_gates
        keys = kv_all[slot, GATE_ROWS:, :]
        for t in range(rows // tile):
            here = slice(t * tile, (t + 1) * tile)
            scores = lax.dot_general(
                qpad[here, :], keys, (((1,), (1,)), ((), ())), preferred_element_type=jnp.float32
            )
            pieces = []
            for j in range(rows // lanes):
                s = scores[:, j * lanes : (j + 1) * lanes] + shift[j : j + 1, :]
                if diagonal:
                    place = lax.broadcasted_iota(jnp.int32, s.shape, 0) + t * tile
                    other = lax.broadcasted_iota(jnp.int32, s.shape, 1) + j * lanes
                    s = jnp.where(other <= place, s, -1e30)
                pieces.append(s)
            most = functools.reduce(jnp.maximum, pieces)
            old = top[here, :]
            new = jnp.maximum(old, jnp.max(most, axis=1, keepdims=True))
            shrink = jnp.exp(old - new)
            raised = [jnp.exp(s - new) for s in pieces]
            total[here, :] = total[here, :] * shrink + functools.reduce(jnp.add, raised)
            weights = jnp.concatenate([r.astype(jnp.bfloat16) for r in raised], axis=1)
            summed[here, :] = summed[here, :] * shrink + jnp.dot(
                weights, keys, preferred_element_type=jnp.float32
            )
            top[here, :] = new

    attend(sp, True)

    def earlier(slot):
        @pl.when(slot < sp)
        def _():
            attend(slot, False)

    def slots(step):
        up_from = lax.rem(chip + chips - step, chips)
        down_from = lax.rem(chip + step, chips)
        return up_from, down_from

    def arrive(slot, step, way, part, target, send):
        hop(slot, step, way, part, target).wait_recv()
        if send is True:
            hop(slot, step, way, part, target).start()
        elif send is not False:

            @pl.when(send)
            def _():
                hop(slot, step, way, part, target).start()

    def partner(step, way, slot):
        share(slot, step, way).wait_recv()
        earlier(slot)

    def both(step):
        up_from, down_from = slots(step)
        before_up, before_down = slots(step - 1)
        up_slot, down_slot = up_from * 2 + core, down_from * 2 + core

        def pieces(these):
            for part in these:
                arrive(up_slot, step, 0, part, up_sp, step < ups)
                arrive(down_slot, step, 1, part, down_sp, step < downs)

        pieces(parts[:2])
        partner(step - 1, 0, before_up * 2 + 1 - core)

        @pl.when(step >= 2)
        def _():
            partner(step - 1, 1, before_down * 2 + 1 - core)

        pieces(parts[2:])
        share(up_slot, step, 0).start()
        share(down_slot, step, 1).start()
        for m in range(2):

            @pl.when(step == max(1, downs - 3 * (1 - m)))
            def _():
                ring_forward(y_size, y, weight_copy(m))

        earlier(up_slot)
        earlier(down_slot)

    if downs >= 1:
        lax.fori_loop(1, downs + 1, lambda i, c: (both(i), c)[1], 0)
    else:
        for m in range(2):
            ring_forward(y_size, y, weight_copy(m))
    last_up, last_down = slots(downs)
    up_from, _ = slots(ups)
    up_slot = up_from * 2 + core
    for part in parts:
        arrive(up_slot, ups, 0, part, up_sp, False)
    share(up_slot, ups, 0).start()
    partner(downs, 0, last_up * 2 + 1 - core)
    if downs >= 1:
        partner(downs, 1, last_down * 2 + 1 - core)
    earlier(up_slot)
    partner(ups, 0, up_from * 2 + 1 - core)

    def finished(lo):
        here = slice(lo, lo + half)
        whole = jnp.sum(total[here, :], axis=1, keepdims=True)
        return summed[here, :] / whole

    left = pltpu.roll(finished(0), size, 1)
    right = finished(half)
    lane = lax.broadcasted_iota(jnp.int32, left.shape, 1)
    att_all[tp] = jnp.where(lane < size, left, right).astype(jnp.bfloat16)

    def give(d):
        return remote(
            att_all.at[tp],
            att_all.at[tp],
            att_send.at[d],
            att_recv.at[tp],
            tp=lax.rem(tp + d, tp_size),
        )

    def take(d):
        owner = lax.rem(tp + tp_size - d, tp_size)
        return remote(
            att_all.at[owner],
            att_all.at[owner],
            att_send.at[d],
            att_recv.at[owner],
            tp=owner,
        )

    for d in range(1, tp_size):
        give(d).start()
    for d in range(1, tp_size):
        take(d).wait_recv()
    weight_start(2)
    projected = jnp.zeros((half, wide.shape[1]), jnp.float32)
    for j in range(tp_size // 2):
        pair = jnp.concatenate([att_all[2 * j], att_all[2 * j + 1]], axis=1)
        projected += jnp.dot(
            pair, wide[j * 4 * size : (j + 1) * 4 * size, :], preferred_element_type=jnp.float32
        )
    for part in range(2):
        here = slice(part * half, (part + 1) * half)
        mixed_v[here, :] = (
            residual_v[here, :].astype(jnp.float32)
            + projected[:, part * columns : (part + 1) * columns]
        ).astype(jnp.bfloat16)


    group = sp_size // y_size
    chunks = 2
    share_rows = 2 * 2 * rows // sp_size // chunks
    height = group * share_rows
    width = tp_size * columns
    hid = y_size * columns
    batch = min(sp_size, max(1, 256 // share_rows))
    span = batch * share_rows

    mixed = mixed_v[...]
    first, second = slot_row[0:1, :], slot_row[1:2, :]

    def near(i):
        j = i // 2
        far = (j + 1) // 2
        odd = j - 2 * (j // 2)
        chip_there = lax.rem(chip + chips + (2 * odd - 1) * far, chips)
        other = i - 2 * j
        return chip_there * 2 + core + other * (1 - 2 * core)

    def send_z(c, i):
        there = near(i)
        return remote(
            outgoing.at[c, there], landed.at[c, sp], z_send.at[c, i], z_recv.at[c, sp], sp=there
        )

    def take_z(c, source):
        return remote(
            outgoing.at[c, sp],
            landed.at[c, source],
            z_send.at[c, 0],
            z_recv.at[c, source],
            sp=source,
        )

    for c in range(chunks):
        for n in range(sp_size // batch):
            start = c * sp_size * share_rows + n * span
            number = lax.broadcasted_iota(jnp.int32, (span, rows), 0) + start
            chosen = jnp.logical_or(number == first, number == second)
            picked = jnp.dot(
                chosen.astype(jnp.float32).astype(jnp.bfloat16),
                mixed,
                preferred_element_type=jnp.float32,
            ).astype(jnp.bfloat16)
            for k in range(batch):
                outgoing[c, n * batch + k] = picked[k * share_rows : (k + 1) * share_rows]
        landed[c, sp] = outgoing[c, sp]
        lax.fori_loop(1, sp_size, lambda i, s: (send_z(c, i).start(), s)[1], 0)

    def give_t(c, i, d, source):
        y_there = source // group
        slot = source - y_there * group
        return remote(
            landed.at[c, source],
            tokens.at[c, slot, tp],
            t_send.at[c, i, d],
            t_recv.at[c],
            tp=y_there * x_size + lax.rem(x + d, x_size),
        )

    def own_t(c, source):
        slot = source - (source // group) * group
        return pltpu.make_async_copy(landed.at[c, source], tokens.at[c, slot, tp], t_recv.at[c])

    def pass_on(c, i, source):
        for d in range(1, x_size):
            give_t(c, i, d, source).start()

        @pl.when(source // group == y)
        def _():
            own_t(c, source).start()

        @pl.when(source // group != y)
        def _():
            give_t(c, i, 0, source).start()

    def arrived(c, i):
        source = near(i)
        take_z(c, source).wait_recv()
        pass_on(c, i, source)

    def h_copy(c):
        def make(owner, k, step, way, index):
            here = hidden.at[c, pl.ds(k * (y_size // 2), y_size // 2), owner]
            return remote(
                here,
                here,
                h_send.at[c, way, index],
                h_recv.at[c, owner, k],
                tp=y * x_size + lax.rem(x + step, x_size),
            )

        return make

    def produce(c):
        pltpu.make_async_copy(tokens.at[c], tokens.at[c], t_recv.at[c]).wait()
        for slot in range(group):
            squares = jnp.zeros((share_rows, columns), jnp.float32)
            for t in range(tp_size):
                piece_t = tokens[c, slot, t].astype(jnp.float32)
                squares += piece_t * piece_t
            scale = lax.rsqrt(jnp.sum(squares, axis=1, keepdims=True) / width + NORM_EPS)
            for t in range(tp_size):
                piece_t = tokens[c, slot, t].astype(jnp.float32)
                normed[
                    slot * share_rows : (slot + 1) * share_rows, t * columns : (t + 1) * columns
                ] = (piece_t * scale * gain_ref[t : t + 1, :]).astype(jnp.bfloat16)
        tile = min(256, hid)
        for n in range(hid // tile):
            cols = slice(n * tile, (n + 1) * tile)
            gate_input = jnp.dot(normed[...], gate_v[:, cols], preferred_element_type=jnp.float32)
            linear_input = jnp.dot(normed[...], up_v[:, cols], preferred_element_type=jnp.float32)
            cut = jnp.minimum(gate_input, CLAMP_LIMIT)
            linear = jnp.clip(linear_input, -CLAMP_LIMIT, CLAMP_LIMIT)
            active = (cut / (1.0 + jnp.exp(-SILU_ALPHA * cut)) * (linear + 1.0)).astype(jnp.bfloat16)
            for k in range(tile // columns):
                hidden[c, n * (tile // columns) + k, x] = active[
                    :, k * columns : (k + 1) * columns
                ]
        ring_start(x_size, x, h_copy(c))


    def arrivals(c, low, high):
        lax.fori_loop(low, high, lambda i, s: (arrived(c, i), s)[1], 0)

    middle = sp_size // 2
    pass_on(0, 0, sp)
    arrivals(0, 1, sp_size)
    ring_forward(y_size, y, weight_copy(2))
    pass_on(1, 0, sp)
    arrivals(1, 1, middle)
    for m in range(2):
        weight_ready(m)
    produce(0)
    arrivals(1, middle, sp_size)
    produce(1)

    def give_y(c, d):
        y_there = lax.rem(y + d, y_size)
        return remote(
            produced.at[c, y_there],
            turned.at[c, y],
            y_send.at[c, d],
            y_recv.at[c, y],
            tp=y_there * x_size + x,
        )

    def take_y(c, d):
        source = lax.rem(y + y_size - d, y_size)
        return source, remote(
            produced.at[c, source],
            turned.at[c, source],
            y_send.at[c, d],
            y_recv.at[c, source],
            tp=source * x_size + x,
        )

    def send_r(c, source, slot):
        there = source * group + slot
        return remote(
            turned.at[c, source, pl.ds(slot * share_rows, share_rows), :],
            returned.at[c, sp],
            r_send.at[c, there],
            r_recv.at[c, sp],
            sp=there,
        )

    def give_back(c, source):
        for slot in range(group):
            there = source * group + slot

            @pl.when(there == sp)
            def _():
                returned[c, sp] = turned[
                    c, source, slot * share_rows : (slot + 1) * share_rows, :
                ]

            @pl.when(there != sp)
            def _():
                send_r(c, source, slot).start()

    for c in range(chunks):
        ring_forward(x_size, x, h_copy(c))
    weight_ready(2)
    for c in range(chunks):
        ring_finish(x_size, x, h_copy(c))
        made = jnp.zeros((height, hid), jnp.float32)
        for t in range(0, tp_size, 2):
            k, j = t // x_size, t % x_size
            pair = jnp.concatenate([hidden[c, k, j], hidden[c, k, j + 1]], axis=1)
            made += jnp.dot(
                pair,
                down_v[t * columns : (t + 2) * columns, :],
                preferred_element_type=jnp.float32,
            )
        for k in range(y_size):
            produced[c, k] = made[:, k * columns : (k + 1) * columns].astype(jnp.bfloat16)
        for d in range(1, y_size):
            give_y(c, d).start()
        turned[c, y] = produced[c, y]
        give_back(c, y)
    for c in range(chunks):
        for d in range(1, y_size):
            source, copy = take_y(c, d)
            copy.wait_recv()
            give_back(c, source)

    sums = [jnp.zeros((rows, columns), jnp.float32) for _ in range(2)]
    for c in range(chunks):
        for n in range(sp_size // batch):
            for k in range(batch):
                e = n * batch + k

                @pl.when(sp != e)
                def _():
                    remote(
                        turned.at[c, 0, pl.ds(0, share_rows), :],
                        returned.at[c, e],
                        r_send.at[c, e],
                        r_recv.at[c, e],
                        sp=sp,
                    ).wait_recv()

            block = jnp.concatenate([returned[c, n * batch + k] for k in range(batch)], axis=0)
            start = c * sp_size * share_rows + n * span
            number = lax.broadcasted_iota(jnp.int32, (rows, span), 1) + start
            for k in range(2):
                chosen = (number == slot_col[:, k : k + 1]).astype(jnp.float32).astype(jnp.bfloat16)
                sums[k] += jnp.dot(chosen, block, preferred_element_type=jnp.float32)
    blended = route_ref[:, 0:1] * sums[0] + route_ref[:, 1:2] * sums[1]
    out_ref[...] = (mixed.astype(jnp.float32) + blended).astype(jnp.bfloat16)

    if ups >= 1:
        for step in range(ups):
            for part in parts:
                hop(sp, step, 0, part, up_sp).wait_send()
        for step in range(downs):
            for part in parts:
                hop(sp, step, 1, part, down_sp).wait_send()
        for step in range(1, ups + 1):
            share(sp, step, 0).wait_send()
        for step in range(1, downs + 1):
            share(sp, step, 1).wait_send()
    share(sp, 0, 0).wait_send()
    for d in range(1, tp_size):
        give(d).wait_send()


    for m in range(3):
        ring_sent(y_size, y, weight_copy(m))
    for c in range(chunks):
        for i in range(1, sp_size):
            send_z(c, i).wait_send()
        for i in range(sp_size):
            for d in range(1, x_size):
                give_t(c, i, d, sp).wait_send()

            @pl.when(near(i) // group != y)
            def _():
                give_t(c, i, 0, sp).wait_send()

        ring_sent(x_size, x, h_copy(c))
        for d in range(1, y_size):
            give_y(c, d).wait_send()
        for e in range(sp_size):

            @pl.when(sp != e)
            def _():
                send_r(c, e // group, e % group).wait_send()


def y_of(tp_size):
    return math.isqrt(tp_size)


def layer(
    mesh,
    query_rows,
    key_rows,
    value_rows,
    cum_gates,
    residual,
    output_weight,
    norm_gain,
    slot,
    route_weights,
    gate_weight,
    up_weight,
    down_weight,
):
    sp_size, tp_size = mesh.shape["sp"], mesh.shape["tp"]
    y_size = y_of(tp_size)
    x_size = tp_size // y_size
    rows, size = query_rows.shape
    columns = output_weight.shape[1]
    group = sp_size // y_size
    depth = gate_weight.shape[1]
    hid = y_size * columns
    part = 2 * rows // sp_size
    height = group * part
    steps = sp_size // 4 + 1
    bf16, f32 = jnp.bfloat16, jnp.float32
    vmem = pl.BlockSpec(memory_space=pltpu.VMEM)
    anywhere = pl.BlockSpec(memory_space=pl.ANY)
    dma = pltpu.SemaphoreType.DMA
    gates = cum_gates.reshape(4, rows // 4)
    return pl.pallas_call(
        functools.partial(layer_kernel, sp_size, tp_size, y_size),
        out_shape=jax.ShapeDtypeStruct((rows, columns), bf16),
        in_specs=[anywhere] * 9 + [vmem] * 4,
        out_specs=vmem,
        scratch_shapes=[
            pltpu.VMEM((size, rows), bf16),
            pltpu.VMEM((size, rows), bf16),
            pltpu.VMEM((size, rows), bf16),
            pltpu.VMEM(gates.shape, f32),
            pltpu.VMEM(residual.shape, bf16),
            pltpu.VMEM(output_weight.shape, bf16),
            pltpu.VMEM((rows, columns), bf16),
            pltpu.VMEM((sp_size, GATE_ROWS + rows, 2 * size), bf16),
            pltpu.VMEM((rows, 2 * size), bf16),
            pltpu.VMEM((tp_size * 2 * size, 2 * columns), bf16),
            pltpu.VMEM((rows, 2 * size), f32),
            pltpu.VMEM((rows, 2 * size), f32),
            pltpu.VMEM((rows, 2 * size), f32),
            pltpu.VMEM((tp_size, rows // 2, 2 * size), bf16),
            pltpu.VMEM((2, sp_size, part, columns), bf16),
            pltpu.VMEM((2, sp_size, part, columns), bf16),
            pltpu.VMEM((2, group, tp_size, part, columns), bf16),
            pltpu.VMEM((height, tp_size * columns), bf16),
            pltpu.VMEM((depth, hid), bf16),
            pltpu.VMEM((depth, hid), bf16),
            pltpu.VMEM((depth, hid), bf16),
            pltpu.VMEM((2, y_size, x_size, height, columns), bf16),
            pltpu.VMEM((2, y_size, height, columns), bf16),
            pltpu.VMEM((2, y_size, height, columns), bf16),
            pltpu.VMEM((2, sp_size, part, columns), bf16),
            dma((6,)),
            dma((sp_size, 4)),
            dma((sp_size,)),
            dma((steps, 2, 4)),
            dma((steps, 2)),
            dma((tp_size,)),
            dma((tp_size,)),
            dma((3,)),
            dma((3, y_size, 2)),
            dma((3, 2, 3)),
            dma((2, sp_size)),
            dma((2, sp_size)),
            dma((2, sp_size, x_size)),
            dma((2,)),
            dma((2, 2, 3)),
            dma((2, x_size, 2)),
            dma((2, y_size)),
            dma((2, y_size)),
            dma((2, sp_size)),
            dma((2, sp_size)),
        ],
        compiler_params=pltpu.CompilerParams(
            collective_id=0, has_side_effects=True, vmem_limit_bytes=60 << 20
        ),
    )(
        query_rows.T,
        key_rows.T,
        value_rows.T,
        gates,
        residual,
        output_weight,
        gate_weight,
        up_weight,
        down_weight,
        slot.T,
        slot,
        route_weights,
        norm_gain.astype(f32).reshape(tp_size, columns),
    )


def slots_of(expert_index, count):
    rows, topk = expert_index.shape
    chosen = expert_index.reshape(rows * topk)
    matches = chosen[:, None] == jnp.arange(count, dtype=jnp.int32)[None, :]
    order = jnp.arange(rows * topk, dtype=jnp.int32)
    before = (order[None, :] < order[:, None]).astype(jnp.bfloat16)
    ahead = jnp.dot(before, matches.astype(jnp.bfloat16), preferred_element_type=jnp.float32)
    rank = jnp.sum(jnp.where(matches, ahead, 0.0), axis=1).astype(jnp.int32)
    part = rows * topk // count
    half = rank // part
    return (half * count * part + chosen * part + rank - half * part).reshape(rows, topk)


def body(
    mesh,
    query_rows,
    key_rows,
    value_rows,
    cum_gates,
    residual,
    output_weight,
    norm_gain,
    expert_index,
    route_weights,
    gate_weight,
    up_weight,
    down_weight,
):
    slot = slots_of(expert_index, mesh.shape["sp"])
    return layer(
        mesh,
        query_rows,
        key_rows,
        value_rows,
        cum_gates,
        residual,
        output_weight,
        norm_gain,
        slot,
        route_weights,
        gate_weight,
        up_weight,
        down_weight,
    )


def solution(mesh):
    placed = (
        P("sp", "tp"),
        P("sp", "tp"),
        P("sp", "tp"),
        P("sp", "tp"),
        P("sp", "tp"),
        P(None, "tp"),
        P(),
        P("sp", None),
        P("sp", None),
        P("sp", None, "tp"),
        P("sp", None, "tp"),
        P("sp", None, "tp"),
    )
    return jax.shard_map(
        functools.partial(body, mesh),
        mesh=mesh,
        in_specs=placed,
        out_specs=P("sp", "tp"),
        check_vma=False,
    )
```

```python
import functools
import math

import jax
import jax.numpy as jnp
from jax import lax
from jax.experimental import pallas as pl
from jax.experimental.pallas import tpu as pltpu
from jax.sharding import PartitionSpec as P

NORM_EPS = 1e-06
CLAMP_LIMIT = 7.0
SILU_ALPHA = 1.702
MESH = pl.DeviceIdType.MESH
GATE_ROWS = 16


def remote(src, dst, send_sem, recv_sem, **where):
    return pltpu.make_async_remote_copy(
        src_ref=src,
        dst_ref=dst,
        send_sem=send_sem,
        recv_sem=recv_sem,
        device_id=where,
        device_id_type=MESH,
    )


def ring_start(n, place, make):
    if n == 4:
        for k in range(2):
            make(place, k, 1, 0, k).start()
            make(place, 1 - k, 3, 1, k).start()
    elif n == 2:
        for k in range(2):
            make(place, k, 1, 0, k).start()


def ring_forward(n, place, make):
    if n == 4:
        before, after = lax.rem(place + 3, 4), lax.rem(place + 1, 4)
        make(before, 0, 1, 0, 2).wait_recv()
        make(before, 0, 1, 0, 2).start()
        make(after, 1, 3, 1, 2).wait_recv()
        make(after, 1, 3, 1, 2).start()


def ring_finish(n, place, make):
    if n == 4:
        make(lax.rem(place + 3, 4), 1, 1, 0, 0).wait_recv()
        make(lax.rem(place + 1, 4), 0, 1, 0, 0).wait_recv()
        for k in range(2):
            make(lax.rem(place + 2, 4), k, 1, 0, 0).wait_recv()
    elif n == 2:
        for k in range(2):
            make(1 - place, k, 1, 0, 0).wait_recv()


def ring_sent(n, place, make):
    if n == 4:
        for k in range(3):
            half = k if k < 2 else 0
            make(place, half, 1, 0, k).wait_send()
            make(place, 1 - half, 3, 1, k).wait_send()
    elif n == 2:
        for k in range(2):
            make(place, k, 1, 0, k).wait_send()


def layer_kernel(
    sp_size,
    tp_size,
    y_size,
    q_ref,
    k_ref,
    v_ref,
    gate_ref,
    residual_ref,
    weight_ref,
    gate_w,
    up_w,
    down_w,
    slot_row,
    slot_col,
    route_ref,
    gain_ref,
    out_ref,
    q_v,
    k_v,
    v_v,
    gate_rows,
    residual_v,
    weight_v,
    mixed_v,
    kv_all,
    qpad,
    wide,
    top,
    total,
    summed,
    att_all,
    outgoing,
    landed,
    tokens,
    normed,
    gate_v,
    up_v,
    down_v,
    hidden,
    produced,
    turned,
    returned,
    in_sem,
    kv_recv,
    own_recv,
    ring_send,
    pair_send,
    att_recv,
    att_send,
    own_w,
    w_recv,
    w_send,
    z_send,
    z_recv,
    t_send,
    t_recv,
    h_send,
    h_recv,
    y_send,
    y_recv,
    r_send,
    r_recv,
):
    chips = sp_size // 2
    ups = chips // 2
    downs = chips - 1 - ups
    sp = lax.axis_index("sp")
    tp = lax.axis_index("tp")
    chip = sp // 2
    core = sp - 2 * chip
    size, rows = q_ref.shape
    half = rows // 2
    x_size = tp_size // y_size
    y = tp // x_size
    x = tp - y * x_size
    quarter = rows // 4
    starts = [0] + [GATE_ROWS + k * quarter for k in range(1, 4)]
    lengths = [GATE_ROWS + quarter] + [quarter] * 3
    parts = range(4)
    up_sp = lax.rem(chip + 1, chips) * 2 + core
    down_sp = lax.rem(chip + chips - 1, chips) * 2 + core
    pair_sp = chip * 2 + 1 - core

    barrier = pltpu.get_barrier_semaphore()
    for target in (up_sp, down_sp, pair_sp):
        pl.semaphore_signal(barrier, inc=1, device_id={"sp": target}, device_id_type=MESH)
    for d in range(1, tp_size):
        pl.semaphore_signal(
            barrier, inc=1, device_id={"tp": lax.rem(tp + d, tp_size)}, device_id_type=MESH
        )

    inputs = [
        pltpu.make_async_copy(source, target, in_sem.at[k])
        for k, (source, target) in enumerate(
            (
                (q_ref, q_v),
                (k_ref, k_v),
                (v_ref, v_v),
                (gate_ref, gate_rows),
                (residual_ref, residual_v),
                (weight_ref, weight_v),
            )
        )
    ]
    for load in inputs:
        load.start()
    for load in inputs[:4]:
        load.wait()

    gates = gate_rows[...]
    high = gates.astype(jnp.bfloat16)
    rest = gates - high.astype(jnp.float32)
    middle = rest.astype(jnp.bfloat16)
    low = (rest - middle.astype(jnp.float32)).astype(jnp.bfloat16)
    kv_all[sp, 0:GATE_ROWS, :] = jnp.concatenate(
        [
            high.astype(jnp.float32),
            middle.astype(jnp.float32),
            low.astype(jnp.float32),
            jnp.zeros_like(gates),
        ],
        axis=0,
    ).astype(jnp.bfloat16)
    both_kv = jnp.concatenate([k_v[...], v_v[...]], axis=0).astype(jnp.float32)
    kv_all[sp, GATE_ROWS:, :] = both_kv.T.astype(jnp.bfloat16)
    qs = q_v[...].astype(jnp.float32) * (size**-0.5)
    qpad[...] = jnp.concatenate([qs, jnp.zeros_like(qs)], axis=0).T.astype(jnp.bfloat16)
    first_gate = gates[0:1, 0:1]

    pl.semaphore_wait(barrier, 3 + tp_size - 1)

    def piece(slot, part):
        return kv_all.at[slot, pl.ds(starts[part], lengths[part]), :]

    def hop(slot, step, way, part, target):
        return remote(
            piece(slot, part),
            piece(slot, part),
            ring_send.at[step, way, part],
            kv_recv.at[slot, part],
            sp=target,
        )

    def share(slot, step, way):
        return remote(
            kv_all.at[slot],
            kv_all.at[slot],
            pair_send.at[step, way],
            own_recv.at[slot],
            sp=pair_sp,
        )

    matrices = ((gate_w, gate_v), (up_w, up_v), (down_w, down_v))
    depth = gate_w.shape[1]
    columns = weight_ref.shape[1]

    def lanes_of(owner):
        return pl.ds(pl.multiple_of(owner * columns, columns), columns)

    def weight_copy(m):
        own, every = matrices[m]

        def make(owner, k, step, way, index):
            here = every.at[pl.ds(k * (depth // 2), depth // 2), lanes_of(owner)]
            mine = own.at[0, pl.ds(k * (depth // 2), depth // 2), :]
            return remote(
                mine if index < 2 else here,
                here,
                w_send.at[m, way, index],
                w_recv.at[m, owner, k],
                tp=lax.rem(y + step, y_size) * x_size + x,
            )

        return make

    def own_weight(m):
        own, every = matrices[m]
        return pltpu.make_async_copy(own.at[0], every.at[:, lanes_of(y)], own_w.at[m])

    def weight_start(m):
        ring_start(y_size, y, weight_copy(m))
        own_weight(m).start()

    def weight_ready(m):
        ring_finish(y_size, y, weight_copy(m))
        own_weight(m).wait()

    if ups >= 1:
        for part in parts:
            hop(sp, 0, 0, part, up_sp).start()
            if downs >= 1:
                hop(sp, 0, 1, part, down_sp).start()
    share(sp, 0, 0).start()
    for m in range(2):
        weight_start(m)
    for load in inputs[4:]:
        load.wait()

    wide[...] = jnp.zeros_like(wide)
    for h in range(tp_size):
        w = weight_v[h * size : (h + 1) * size, :]
        wide[h * 2 * size : h * 2 * size + size, 0 : w.shape[1]] = w
        wide[h * 2 * size + size : (h + 1) * 2 * size, w.shape[1] :] = w

    top[...] = jnp.full_like(top, -1e30)
    total[...] = jnp.zeros_like(total)
    summed[...] = jnp.zeros_like(summed)
    tile = rows
    lanes = 128

    def attend(slot, diagonal):
        parts = kv_all[slot, 0:GATE_ROWS, :].astype(jnp.float32)
        n4 = GATE_ROWS // 4
        key_gates = parts[0:n4] + parts[n4 : 2 * n4] + parts[2 * n4 : 3 * n4]
        shift = first_gate - key_gates
        keys = kv_all[slot, GATE_ROWS:, :]
        for t in range(rows // tile):
            here = slice(t * tile, (t + 1) * tile)
            scores = lax.dot_general(
                qpad[here, :], keys, (((1,), (1,)), ((), ())), preferred_element_type=jnp.float32
            )
            pieces = []
            for j in range(rows // lanes):
                s = scores[:, j * lanes : (j + 1) * lanes] + shift[j : j + 1, :]
                if diagonal:
                    place = lax.broadcasted_iota(jnp.int32, s.shape, 0) + t * tile
                    other = lax.broadcasted_iota(jnp.int32, s.shape, 1) + j * lanes
                    s = jnp.where(other <= place, s, -1e30)
                pieces.append(s)
            most = functools.reduce(jnp.maximum, pieces)
            old = top[here, :]
            new = jnp.maximum(old, jnp.max(most, axis=1, keepdims=True))
            shrink = jnp.exp(old - new)
            raised = [jnp.exp(s - new) for s in pieces]
            total[here, :] = total[here, :] * shrink + functools.reduce(jnp.add, raised)
            weights = jnp.concatenate([r.astype(jnp.bfloat16) for r in raised], axis=1)
            summed[here, :] = summed[here, :] * shrink + jnp.dot(
                weights, keys, preferred_element_type=jnp.float32
            )
            top[here, :] = new

    attend(sp, True)

    def earlier(slot):
        @pl.when(slot < sp)
        def _():
            attend(slot, False)

    def slots(step):
        up_from = lax.rem(chip + chips - step, chips)
        down_from = lax.rem(chip + step, chips)
        return up_from, down_from

    def arrive(slot, step, way, part, target, send):
        hop(slot, step, way, part, target).wait_recv()
        if send is True:
            hop(slot, step, way, part, target).start()
        elif send is not False:

            @pl.when(send)
            def _():
                hop(slot, step, way, part, target).start()

    def partner(step, way, slot):
        share(slot, step, way).wait_recv()
        earlier(slot)

    def both(step):
        up_from, down_from = slots(step)
        before_up, before_down = slots(step - 1)
        up_slot, down_slot = up_from * 2 + core, down_from * 2 + core

        def pieces(these):
            for part in these:
                arrive(up_slot, step, 0, part, up_sp, step < ups)
                arrive(down_slot, step, 1, part, down_sp, step < downs)

        pieces(parts[:2])
        partner(step - 1, 0, before_up * 2 + 1 - core)

        @pl.when(step >= 2)
        def _():
            partner(step - 1, 1, before_down * 2 + 1 - core)

        pieces(parts[2:])
        share(up_slot, step, 0).start()
        share(down_slot, step, 1).start()
        for m in range(2):

            @pl.when(step == max(1, downs - 3 * (1 - m)))
            def _():
                ring_forward(y_size, y, weight_copy(m))

        earlier(up_slot)
        earlier(down_slot)

    if downs >= 1:
        lax.fori_loop(1, downs + 1, lambda i, c: (both(i), c)[1], 0)
    else:
        for m in range(2):
            ring_forward(y_size, y, weight_copy(m))
    last_up, last_down = slots(downs)
    up_from, _ = slots(ups)
    up_slot = up_from * 2 + core
    for part in parts:
        arrive(up_slot, ups, 0, part, up_sp, False)
    share(up_slot, ups, 0).start()
    partner(downs, 0, last_up * 2 + 1 - core)
    if downs >= 1:
        partner(downs, 1, last_down * 2 + 1 - core)
    earlier(up_slot)
    partner(ups, 0, up_from * 2 + 1 - core)

    def finished(lo):
        here = slice(lo, lo + half)
        whole = jnp.sum(total[here, :], axis=1, keepdims=True)
        return summed[here, :] / whole

    left = pltpu.roll(finished(0), size, 1)
    right = finished(half)
    lane = lax.broadcasted_iota(jnp.int32, left.shape, 1)
    att_all[tp] = jnp.where(lane < size, left, right).astype(jnp.bfloat16)

    def give(d):
        return remote(
            att_all.at[tp],
            att_all.at[tp],
            att_send.at[d],
            att_recv.at[tp],
            tp=lax.rem(tp + d, tp_size),
        )

    def take(d):
        owner = lax.rem(tp + tp_size - d, tp_size)
        return remote(
            att_all.at[owner],
            att_all.at[owner],
            att_send.at[d],
            att_recv.at[owner],
            tp=owner,
        )

    for d in range(1, tp_size):
        give(d).start()
    for d in range(1, tp_size):
        take(d).wait_recv()
    weight_start(2)
    projected = jnp.zeros((half, wide.shape[1]), jnp.float32)
    for j in range(tp_size // 2):
        pair = jnp.concatenate([att_all[2 * j], att_all[2 * j + 1]], axis=1)
        projected += jnp.dot(
            pair, wide[j * 4 * size : (j + 1) * 4 * size, :], preferred_element_type=jnp.float32
        )
    for part in range(2):
        here = slice(part * half, (part + 1) * half)
        mixed_v[here, :] = (
            residual_v[here, :].astype(jnp.float32)
            + projected[:, part * columns : (part + 1) * columns]
        ).astype(jnp.bfloat16)


    group = sp_size // y_size
    chunks = 2
    share_rows = 2 * 2 * rows // sp_size // chunks
    height = group * share_rows
    width = tp_size * columns
    hid = y_size * columns
    batch = min(sp_size, max(1, 256 // share_rows))
    span = batch * share_rows

    mixed = mixed_v[...]
    first, second = slot_row[0:1, :], slot_row[1:2, :]

    def near(i):
        j = i // 2
        far = (j + 1) // 2
        odd = j - 2 * (j // 2)
        chip_there = lax.rem(chip + chips + (2 * odd - 1) * far, chips)
        other = i - 2 * j
        return chip_there * 2 + core + other * (1 - 2 * core)

    def send_z(c, i):
        there = near(i)
        return remote(
            outgoing.at[c, there], landed.at[c, sp], z_send.at[c, i], z_recv.at[c, sp], sp=there
        )

    def take_z(c, source):
        return remote(
            outgoing.at[c, sp],
            landed.at[c, source],
            z_send.at[c, 0],
            z_recv.at[c, source],
            sp=source,
        )

    for c in range(chunks):
        for n in range(sp_size // batch):
            start = c * sp_size * share_rows + n * span
            number = lax.broadcasted_iota(jnp.int32, (span, rows), 0) + start
            chosen = jnp.logical_or(number == first, number == second)
            picked = jnp.dot(
                chosen.astype(jnp.float32).astype(jnp.bfloat16),
                mixed,
                preferred_element_type=jnp.float32,
            ).astype(jnp.bfloat16)
            for k in range(batch):
                outgoing[c, n * batch + k] = picked[k * share_rows : (k + 1) * share_rows]
        landed[c, sp] = outgoing[c, sp]
        lax.fori_loop(1, sp_size, lambda i, s: (send_z(c, sp_size - i).start(), s)[1], 0)

    def give_t(c, i, d, source):
        y_there = source // group
        slot = source - y_there * group
        return remote(
            landed.at[c, source],
            tokens.at[c, slot, tp],
            t_send.at[c, i, d],
            t_recv.at[c],
            tp=y_there * x_size + lax.rem(x + d, x_size),
        )

    def own_t(c, source):
        slot = source - (source // group) * group
        return pltpu.make_async_copy(landed.at[c, source], tokens.at[c, slot, tp], t_recv.at[c])

    def pass_on(c, i, source):
        for d in range(1, x_size):
            give_t(c, i, d, source).start()

        @pl.when(source // group == y)
        def _():
            own_t(c, source).start()

        @pl.when(source // group != y)
        def _():
            give_t(c, i, 0, source).start()

    def arrived(c, i):
        source = near(i)
        take_z(c, source).wait_recv()
        pass_on(c, i, source)

    def h_copy(c):
        def make(owner, k, step, way, index):
            here = hidden.at[c, pl.ds(k * (y_size // 2), y_size // 2), owner]
            return remote(
                here,
                here,
                h_send.at[c, way, index],
                h_recv.at[c, owner, k],
                tp=y * x_size + lax.rem(x + step, x_size),
            )

        return make

    def produce(c):
        pltpu.make_async_copy(tokens.at[c], tokens.at[c], t_recv.at[c]).wait()
        for slot in range(group):
            squares = jnp.zeros((share_rows, columns), jnp.float32)
            for t in range(tp_size):
                piece_t = tokens[c, slot, t].astype(jnp.float32)
                squares += piece_t * piece_t
            scale = lax.rsqrt(jnp.sum(squares, axis=1, keepdims=True) / width + NORM_EPS)
            for t in range(tp_size):
                piece_t = tokens[c, slot, t].astype(jnp.float32)
                normed[
                    slot * share_rows : (slot + 1) * share_rows, t * columns : (t + 1) * columns
                ] = (piece_t * scale * gain_ref[t : t + 1, :]).astype(jnp.bfloat16)
        tile = min(256, hid)
        for n in range(hid // tile):
            cols = slice(n * tile, (n + 1) * tile)
            gate_input = jnp.dot(normed[...], gate_v[:, cols], preferred_element_type=jnp.float32)
            linear_input = jnp.dot(normed[...], up_v[:, cols], preferred_element_type=jnp.float32)
            cut = jnp.minimum(gate_input, CLAMP_LIMIT)
            linear = jnp.clip(linear_input, -CLAMP_LIMIT, CLAMP_LIMIT)
            active = (cut / (1.0 + jnp.exp(-SILU_ALPHA * cut)) * (linear + 1.0)).astype(jnp.bfloat16)
            for k in range(tile // columns):
                hidden[c, n * (tile // columns) + k, x] = active[
                    :, k * columns : (k + 1) * columns
                ]
        ring_start(x_size, x, h_copy(c))


    def arrivals(c, low, high):
        lax.fori_loop(low, high, lambda i, s: (arrived(c, sp_size - i), s)[1], 0)

    middle = sp_size // 2
    pass_on(0, 0, sp)
    arrivals(0, 1, sp_size)
    ring_forward(y_size, y, weight_copy(2))
    pass_on(1, 0, sp)
    arrivals(1, 1, middle)
    for m in range(2):
        weight_ready(m)
    produce(0)
    arrivals(1, middle, sp_size)
    produce(1)

    def give_y(c, d):
        y_there = lax.rem(y + d, y_size)
        return remote(
            produced.at[c, y_there],
            turned.at[c, y],
            y_send.at[c, d],
            y_recv.at[c, y],
            tp=y_there * x_size + x,
        )

    def take_y(c, d):
        source = lax.rem(y + y_size - d, y_size)
        return source, remote(
            produced.at[c, source],
            turned.at[c, source],
            y_send.at[c, d],
            y_recv.at[c, source],
            tp=source * x_size + x,
        )

    def row_of(slot):
        return pl.multiple_of(slot * share_rows, share_rows)

    def send_r(c, source, slot):
        there = source * group + slot
        return remote(
            turned.at[c, source, pl.ds(row_of(slot), share_rows), :],
            returned.at[c, sp],
            r_send.at[c, there],
            r_recv.at[c, sp],
            sp=there,
        )

    def give_back(c, source):
        for k in range(group):
            slot = lax.rem(sp + k, group)
            there = source * group + slot

            @pl.when(there == sp)
            def _():
                returned[c, sp] = turned[
                    c, source, pl.ds(row_of(slot), share_rows), :
                ]

            @pl.when(there != sp)
            def _():
                send_r(c, source, slot).start()

    for c in range(chunks):
        ring_forward(x_size, x, h_copy(c))
    weight_ready(2)
    for c in range(chunks):
        ring_finish(x_size, x, h_copy(c))
        made = jnp.zeros((height, hid), jnp.float32)
        for t in range(0, tp_size, 2):
            k, j = t // x_size, t % x_size
            pair = jnp.concatenate([hidden[c, k, j], hidden[c, k, j + 1]], axis=1)
            made += jnp.dot(
                pair,
                down_v[t * columns : (t + 2) * columns, :],
                preferred_element_type=jnp.float32,
            )
        for k in range(y_size):
            produced[c, k] = made[:, k * columns : (k + 1) * columns].astype(jnp.bfloat16)
        for d in range(1, y_size):
            give_y(c, d).start()
        turned[c, y] = produced[c, y]
        give_back(c, y)
    for c in range(chunks):
        for d in range(1, y_size):
            source, copy = take_y(c, d)
            copy.wait_recv()
            give_back(c, source)

    sums = [jnp.zeros((rows, columns), jnp.float32) for _ in range(2)]
    for c in range(chunks):
        for n in range(sp_size // batch):
            for k in range(batch):
                e = n * batch + k

                @pl.when(sp != e)
                def _():
                    remote(
                        turned.at[c, 0, pl.ds(0, share_rows), :],
                        returned.at[c, e],
                        r_send.at[c, e],
                        r_recv.at[c, e],
                        sp=sp,
                    ).wait_recv()

            block = jnp.concatenate([returned[c, n * batch + k] for k in range(batch)], axis=0)
            start = c * sp_size * share_rows + n * span
            number = lax.broadcasted_iota(jnp.int32, (rows, span), 1) + start
            for k in range(2):
                chosen = (number == slot_col[:, k : k + 1]).astype(jnp.float32).astype(jnp.bfloat16)
                sums[k] += jnp.dot(chosen, block, preferred_element_type=jnp.float32)
    blended = route_ref[:, 0:1] * sums[0] + route_ref[:, 1:2] * sums[1]
    out_ref[...] = (mixed.astype(jnp.float32) + blended).astype(jnp.bfloat16)

    if ups >= 1:
        for step in range(ups):
            for part in parts:
                hop(sp, step, 0, part, up_sp).wait_send()
        for step in range(downs):
            for part in parts:
                hop(sp, step, 1, part, down_sp).wait_send()
        for step in range(1, ups + 1):
            share(sp, step, 0).wait_send()
        for step in range(1, downs + 1):
            share(sp, step, 1).wait_send()
    share(sp, 0, 0).wait_send()
    for d in range(1, tp_size):
        give(d).wait_send()


    for m in range(3):
        ring_sent(y_size, y, weight_copy(m))
    for c in range(chunks):
        for i in range(1, sp_size):
            send_z(c, i).wait_send()
        for i in range(sp_size):
            for d in range(1, x_size):
                give_t(c, i, d, sp).wait_send()

            @pl.when(near(i) // group != y)
            def _():
                give_t(c, i, 0, sp).wait_send()

        ring_sent(x_size, x, h_copy(c))
        for d in range(1, y_size):
            give_y(c, d).wait_send()
        for e in range(sp_size):

            @pl.when(sp != e)
            def _():
                send_r(c, e // group, e % group).wait_send()


def y_of(tp_size):
    return math.isqrt(tp_size)


def layer(
    mesh,
    query_rows,
    key_rows,
    value_rows,
    cum_gates,
    residual,
    output_weight,
    norm_gain,
    slot,
    route_weights,
    gate_weight,
    up_weight,
    down_weight,
):
    sp_size, tp_size = mesh.shape["sp"], mesh.shape["tp"]
    y_size = y_of(tp_size)
    x_size = tp_size // y_size
    rows, size = query_rows.shape
    columns = output_weight.shape[1]
    group = sp_size // y_size
    depth = gate_weight.shape[1]
    hid = y_size * columns
    part = 2 * rows // sp_size
    height = group * part
    steps = sp_size // 4 + 1
    bf16, f32 = jnp.bfloat16, jnp.float32
    vmem = pl.BlockSpec(memory_space=pltpu.VMEM)
    anywhere = pl.BlockSpec(memory_space=pl.ANY)
    dma = pltpu.SemaphoreType.DMA
    gates = cum_gates.reshape(4, rows // 4)
    return pl.pallas_call(
        functools.partial(layer_kernel, sp_size, tp_size, y_size),
        out_shape=jax.ShapeDtypeStruct((rows, columns), bf16),
        in_specs=[anywhere] * 9 + [vmem] * 4,
        out_specs=vmem,
        scratch_shapes=[
            pltpu.VMEM((size, rows), bf16),
            pltpu.VMEM((size, rows), bf16),
            pltpu.VMEM((size, rows), bf16),
            pltpu.VMEM(gates.shape, f32),
            pltpu.VMEM(residual.shape, bf16),
            pltpu.VMEM(output_weight.shape, bf16),
            pltpu.VMEM((rows, columns), bf16),
            pltpu.VMEM((sp_size, GATE_ROWS + rows, 2 * size), bf16),
            pltpu.VMEM((rows, 2 * size), bf16),
            pltpu.VMEM((tp_size * 2 * size, 2 * columns), bf16),
            pltpu.VMEM((rows, 2 * size), f32),
            pltpu.VMEM((rows, 2 * size), f32),
            pltpu.VMEM((rows, 2 * size), f32),
            pltpu.VMEM((tp_size, rows // 2, 2 * size), bf16),
            pltpu.VMEM((2, sp_size, part, columns), bf16),
            pltpu.VMEM((2, sp_size, part, columns), bf16),
            pltpu.VMEM((2, group, tp_size, part, columns), bf16),
            pltpu.VMEM((height, tp_size * columns), bf16),
            pltpu.VMEM((depth, hid), bf16),
            pltpu.VMEM((depth, hid), bf16),
            pltpu.VMEM((depth, hid), bf16),
            pltpu.VMEM((2, y_size, x_size, height, columns), bf16),
            pltpu.VMEM((2, y_size, height, columns), bf16),
            pltpu.VMEM((2, y_size, height, columns), bf16),
            pltpu.VMEM((2, sp_size, part, columns), bf16),
            dma((6,)),
            dma((sp_size, 4)),
            dma((sp_size,)),
            dma((steps, 2, 4)),
            dma((steps, 2)),
            dma((tp_size,)),
            dma((tp_size,)),
            dma((3,)),
            dma((3, y_size, 2)),
            dma((3, 2, 3)),
            dma((2, sp_size)),
            dma((2, sp_size)),
            dma((2, sp_size, x_size)),
            dma((2,)),
            dma((2, 2, 3)),
            dma((2, x_size, 2)),
            dma((2, y_size)),
            dma((2, y_size)),
            dma((2, sp_size)),
            dma((2, sp_size)),
        ],
        compiler_params=pltpu.CompilerParams(
            collective_id=0, has_side_effects=True, vmem_limit_bytes=60 << 20
        ),
    )(
        query_rows.T,
        key_rows.T,
        value_rows.T,
        gates,
        residual,
        output_weight,
        gate_weight,
        up_weight,
        down_weight,
        slot.T,
        slot,
        route_weights,
        norm_gain.astype(f32).reshape(tp_size, columns),
    )


def slots_of(expert_index, count):
    rows, topk = expert_index.shape
    chosen = expert_index.reshape(rows * topk)
    matches = chosen[:, None] == jnp.arange(count, dtype=jnp.int32)[None, :]
    order = jnp.arange(rows * topk, dtype=jnp.int32)
    before = (order[None, :] < order[:, None]).astype(jnp.bfloat16)
    ahead = jnp.dot(before, matches.astype(jnp.bfloat16), preferred_element_type=jnp.float32)
    rank = jnp.sum(jnp.where(matches, ahead, 0.0), axis=1).astype(jnp.int32)
    part = rows * topk // count
    half = rank // part
    return (half * count * part + chosen * part + rank - half * part).reshape(rows, topk)


def body(
    mesh,
    query_rows,
    key_rows,
    value_rows,
    cum_gates,
    residual,
    output_weight,
    norm_gain,
    expert_index,
    route_weights,
    gate_weight,
    up_weight,
    down_weight,
):
    slot = slots_of(expert_index, mesh.shape["sp"])
    return layer(
        mesh,
        query_rows,
        key_rows,
        value_rows,
        cum_gates,
        residual,
        output_weight,
        norm_gain,
        slot,
        route_weights,
        gate_weight,
        up_weight,
        down_weight,
    )


def solution(mesh):
    placed = (
        P("sp", "tp"),
        P("sp", "tp"),
        P("sp", "tp"),
        P("sp", "tp"),
        P("sp", "tp"),
        P(None, "tp"),
        P(),
        P("sp", None),
        P("sp", None),
        P("sp", None, "tp"),
        P("sp", None, "tp"),
        P("sp", None, "tp"),
    )
    return jax.shard_map(
        functools.partial(body, mesh),
        mesh=mesh,
        in_specs=placed,
        out_specs=P("sp", "tp"),
        check_vma=False,
    )
```
